128 devices in a mesh: ep: 16 (over z, x), tp: 8 (over y, core).
Axes of the slice: x: 4, y: 4, z: 4, core: 2. Of those that a mesh axis runs over, the one named last changes fastest.
Arguments:
- mix_tokens: bfloat16 [16384, 2048], P('ep'), may hold values from -6 to 6
- mix_gain: float32 [2048], replicated, may hold values from 0.1 to 1.9
- w_query: bfloat16 [2048, 2048], P(None, 'tp'), may hold values from -0.125 to 0.125
- w_forget_fwd: bfloat16 [2048, 2048], P(None, 'tp'), may hold values from -0.125 to 0.125
- w_forget_bwd: bfloat16 [2048, 2048], P(None, 'tp'), may hold values from -0.125 to 0.125
- w_value: bfloat16 [2048, 2048], P(None, 'tp'), may hold values from -0.125 to 0.125
- decay_floor: float32 [2048], P('tp'), may hold values from 0.975 to 1
- decay_shift: float32 [16384, 16], P('ep', 'tp'), may hold values from -1.3 to 0
- head_gain: float32 [128], replicated, may hold values from 0.1 to 1.9
- w_out: bfloat16 [2048, 2048], replicated, may hold values from -0.125 to 0.125
- moe_tokens: bfloat16 [6144, 2048], P('ep'), may hold values from -6 to 6
- moe_gain: float32 [2048], replicated, may hold values from 0.1 to 1.9
- routes: int32 [6144, 2], P('ep'), may hold values from 0 to 15, all different within a row; in each aligned block of 384 rows (0 to 383, 384 to 767, ...) at most 72 rows name the same one
- route_logits: float32 [6144, 2], P('ep'), may hold values from -6 to 6
- w_expert_gate: bfloat16 [16, 2048, 5120], P('ep', None, 'tp'), may hold values from -0.125 to 0.125
- w_expert_up: bfloat16 [16, 2048, 5120], P('ep', None, 'tp'), may hold values from -0.125 to 0.125
- w_expert_down: bfloat16 [16, 5120, 2048], P('ep', 'tp'), may hold values from -0.078125 to 0.078125
Outputs:
- mixed_out: bfloat16 [16384, 2048], P(('ep', 'tp'))
- moe_out: bfloat16 [6144, 2048], P('ep', 'tp')
The draws below stay inside these ranges and needn't reach their ends.
Inputs may be any that keep to these rules, and one draw needn't show every extreme that they name: `routes`: in each aligned block of 384 rows (the rows of one index of ep) no expert is named by more than 72 rows, and in some block an expert is named by exactly 72; the two entries of a row differ.
All inputs are finite; a program needn't handle non-finite values.
Results may differ from the reference program's by a relative error of at most 0.014.
Values may be sent and summed in bfloat16 or wider, within the bound.
No kernel may reach another device: no remote copies, remote signals or barrier semaphores. Data moves between devices by JAX's collectives and lax.ppermute only.
A program may use at most 128 MiB of HBM per device.

```python
import functools
import math
import jax
import jax.numpy as jnp
import numpy as np
from jax import lax

D = 2048
HEADS = 16
DK = 128
DV = 128
FF = 5120
TOPK = 2
M_EP = 384
SEG = 1024
ROWS = 16384
MROWS = 6144
EXPERTS = 16
CAP = 72
N_EP = 16
N_TP = 8


def decay_table(key):
    head_key = jax.random.fold_in(key, 11)
    scores = jax.random.randint(jax.random.fold_in(head_key, 1), (HEADS,), 0, 1000)
    forced = jax.random.randint(jax.random.fold_in(head_key, 2), (), 0, HEADS)
    limit = 500
    return (scores < limit) | (jnp.arange(HEADS) == forced)


def draw_decay_floor(key, part):
    fast = decay_table(key)
    rate = jnp.where(fast, 1.0 / 40.0, 0.2 / ROWS).astype(jnp.float32)
    spread = jax.random.uniform(jax.random.fold_in(key, 21), (HEADS, DK), jnp.float32, 0.5, 1.0)
    return (1.0 - rate[:, None] * spread).reshape(HEADS * DK)


def draw_decay_shift(key, part):
    fast = decay_table(key)
    start_offset = jnp.where(fast, 1.0 / 40.0, 0.25 / ROWS).astype(jnp.float32)
    block_total = ROWS // SEG
    factor = jnp.exp(jax.random.uniform(jax.random.fold_in(key, 31), (block_total, HEADS), jnp.float32, math.log(0.5), math.log(2.0)))
    row_amounts = jnp.repeat(factor, SEG, axis=0)
    slot_locations = jax.random.randint(jax.random.fold_in(key, 32), (2, HEADS), 0, ROWS)
    loss_values = jax.random.uniform(jax.random.fold_in(key, 33), (2, HEADS), jnp.float32, 0.2, 0.45)
    row_identifiers = jnp.arange(ROWS)[:, None]
    token_groups = jnp.where(row_identifiers == slot_locations[0][None, :], jnp.log1p(-loss_values[0])[None, :], 0.0) + jnp.where(row_identifiers == slot_locations[1][None, :], jnp.log1p(-loss_values[1])[None, :], 0.0)
    return (-start_offset[None, :] * row_amounts + token_groups).astype(jnp.float32)


def block_levels(rng, shape, shards, low, top_value):
    def one(dim, blocks):
        heights = jax.random.uniform(jax.random.fold_in(jax.random.fold_in(rng, 6), dim), (blocks,), jnp.float32, low / len(shards), top_value / len(shards))
        return jnp.repeat(jnp.exp(heights), shape[dim] // blocks).reshape((-1,) + (1,) * (len(shape) - dim - 1))

    loudness = one(*shards[0])
    for cut in shards[1:]:
        loudness = loudness * one(*cut)
    return loudness


def shared_out(own_key, own, number, rows, number_of, top, bound, skew):
    ranking = jax.random.permutation(own_key, number_of)
    packed, common = load_shares(number_of, rows * top, bound, skew, True), load_shares(number_of, rows * top, bound, skew, False)
    places = jnp.arange(number_of)

    def named(lengths, offset_by):
        used = int((lengths > 0).sum())
        fixed = max(1, used // 4)
        passed = fixed + (places - fixed + offset_by * (used - fixed)) % max(1, number_of - fixed)
        return jnp.zeros((number_of,), jnp.int32).at[ranking[jnp.where(places < fixed, places, passed)]].set(jnp.asarray(lengths, jnp.int32))

    lengths = jnp.where(number % 4 == 0, named(packed, number // 4), named(common, number - number // 4 - 1))
    mixed = jax.random.permutation(jax.random.fold_in(own, 3), number_of)
    donor, sink = mixed[0:number_of // 2 * 2:2], mixed[1:number_of // 2 * 2:2]
    slack = jnp.minimum(lengths[donor] - 1, bound - lengths[sink]) // 2
    slack = jnp.where((donor == ranking[0]) | (sink == ranking[0]) | (lengths[sink] == 0), 0, jnp.maximum(slack, 0))
    passed = jax.random.randint(jax.random.fold_in(own, 4), (number_of // 2,), 0, 1 << 20) % (slack + 1)
    lengths = lengths.at[donor].add(-passed).at[sink].add(passed)
    labels = jnp.searchsorted(jnp.cumsum(lengths), jnp.arange(rows * top), side="right").astype(jnp.int32)
    listing = labels.reshape(top, rows).T
    listing = listing[jax.random.permutation(jax.random.fold_in(own, 1), rows)]
    offset_by = jax.random.randint(jax.random.fold_in(own, 2), (rows, 1), 0, top)
    return jnp.take_along_axis(listing, (jnp.arange(top)[None, :] + offset_by) % top, axis=1)


def load_shares(count, total, reach, lean, full):
    portions = [(1 << 20) // math.isqrt(rank ** lean) + 1 for rank in range(1, count + 1)]
    largest = reach if full else min(reach, max(-(-total // count), total * portions[0] // sum(portions)))
    least = 1 if total - largest >= count - 1 else 0
    holding, surplus = [largest] + [least] * (count - 1), total - largest - least * (count - 1)
    while surplus > 0:
        free = [i for i in range(1, count) if holding[i] < largest] or [i for i in range(1, count) if holding[i] < reach]
        whole, remaining = sum([portions[i] for i in free]), surplus
        for i in free:
            more = min(reach - holding[i], max(1, remaining * portions[i] // whole), surplus)
            holding[i] = holding[i] + more
            surplus = surplus - more
    return np.array(holding)


def gaussian(key, shape, scale, most, cuts=(), held_as=jnp.bfloat16):
    values = scale * jax.random.normal(key, shape, jnp.float32)
    if cuts:
        values = values * block_levels(key, shape, cuts, -0.22, 0.18)
    return jnp.clip(values, -most, most).astype(held_as)


def setup_inputs(seed: int = 0) -> dict:
    splits = jax.random.split(jax.random.key(seed), 18)
    mix_tokens = gaussian(splits[0], (ROWS, D), 1.0, 6.0, ((0, 16),))
    mix_gain = jnp.clip(1.0 + 0.18 * jax.random.normal(splits[1], (D,), jnp.float32), 0.1, 1.9)
    w_query = gaussian(splits[2], (D, HEADS * DK), D ** -0.5, 0.125, ((1, 8),))
    w_forget_fwd = gaussian(splits[3], (D, HEADS * DK), D ** -0.5, 0.125, ((1, 8),))
    w_forget_bwd = gaussian(splits[4], (D, HEADS * DK), D ** -0.5, 0.125, ((1, 8),))
    w_value = gaussian(splits[5], (D, HEADS * DV), D ** -0.5, 0.125, ((1, 8),))
    decay_floor = draw_decay_floor(jax.random.fold_in(splits[17], 71), 0)
    decay_shift = draw_decay_shift(jax.random.fold_in(splits[17], 71), 0)
    head_gain = jnp.clip(1.0 + 0.18 * jax.random.normal(splits[8], (DV,), jnp.float32), 0.1, 1.9)
    w_out = gaussian(splits[9], (HEADS * DV, D), D ** -0.5, 0.125)
    moe_tokens = gaussian(splits[10], (MROWS, D), 1.0, 6.0, ((0, 16),))
    moe_gain = jnp.clip(1.0 + 0.18 * jax.random.normal(splits[11], (D,), jnp.float32), 0.1, 1.9)
    routes_keys = jax.random.split(jax.random.fold_in(splits[12], 1), MROWS // M_EP)
    routes_turns = jax.random.permutation(jax.random.fold_in(splits[12], 3), MROWS // M_EP)
    routes = jax.vmap(lambda own, number: shared_out(jax.random.fold_in(splits[12], 2), own, number, M_EP, EXPERTS, 2, CAP, 1))(routes_keys, routes_turns).reshape((MROWS, TOPK))
    route_logits = gaussian(splits[13], (MROWS, TOPK), 1.5, 6.0, ((0, 16),), jnp.float32)
    w_expert_gate = gaussian(splits[14], (EXPERTS, D, FF), D ** -0.5, 0.125, ((0, 16), (2, 8)))
    w_expert_up = gaussian(splits[15], (EXPERTS, D, FF), D ** -0.5, 0.125, ((0, 16), (2, 8)))
    w_expert_down = gaussian(splits[16], (EXPERTS, FF, D), FF ** -0.5, 0.078125, ((0, 16), (1, 8)))
    return {"mix_tokens": mix_tokens, "mix_gain": mix_gain, "w_query": w_query, "w_forget_fwd": w_forget_fwd, "w_forget_bwd": w_forget_bwd, "w_value": w_value, "decay_floor": decay_floor, "decay_shift": decay_shift, "head_gain": head_gain, "w_out": w_out, "moe_tokens": moe_tokens, "moe_gain": moe_gain, "routes": routes, "route_logits": route_logits, "w_expert_gate": w_expert_gate, "w_expert_up": w_expert_up, "w_expert_down": w_expert_down}


EPSILON = 1e-06
PRECISE = lax.Precision.HIGHEST

def rms_rows(array, norm_gain):
    floats = array.astype(jnp.float32)
    factor = lax.rsqrt(lax.optimization_barrier(jnp.mean(floats * floats, axis=-1, keepdims=True)) + EPSILON)
    return floats * factor * norm_gain

def decay_terms(pre_act, lower_bound, shifts, head_count):
    squashed = jax.nn.sigmoid(pre_act.astype(jnp.float32))
    key_rows = (1.0 - lower_bound)[None, :] * (1.0 - squashed)
    key_rows = key_rows.reshape(key_rows.shape[0], head_count, key_rows.shape[1] // head_count)
    log_decay = jnp.log1p(-key_rows) + shifts[:, :, None]
    return (key_rows, log_decay)

def sweep_blocks(queries, key_rows, values, log_decay, blk_rows):
    token_count, head_count, key_width = queries.shape
    value_width = values.shape[2]
    block_count = token_count // blk_rows
    lower_mask = jnp.tril(jnp.ones((blk_rows, blk_rows), jnp.float32))

    def to_blocks(array):
        return array.reshape(block_count, blk_rows, head_count, array.shape[2])

    def advance(carried, block):
        states, offset = carried
        block_q, block_k, block_v, block_g = block
        running = jnp.cumsum(block_g, axis=0)
        query_grown = block_q * jnp.exp(running)
        key_shrunk = block_k * jnp.exp(-running)
        scores = jnp.einsum('thd,shd->hts', query_grown, key_shrunk, precision=PRECISE) * lower_mask[None]
        result = jnp.einsum('hts,shv->thv', scores, block_v, precision=PRECISE) + jnp.einsum('thd,hdv->thv', query_grown, states, precision=PRECISE)
        block_end = running[-1]
        states = jnp.exp(block_end)[:, :, None] * states + jnp.einsum('shd,shv->hdv', block_k * jnp.exp(block_end[None] - running), block_v, precision=PRECISE)
        return ((states, offset + block_end), (result, offset[None] + running))
    starting = (jnp.zeros((head_count, key_width, value_width), jnp.float32), jnp.zeros((head_count, key_width), jnp.float32))
    blocks_in = (to_blocks(queries), to_blocks(key_rows), to_blocks(values), to_blocks(log_decay))
    (states, totals), (results, cumulative) = lax.scan(advance, starting, blocks_in)
    return (results.reshape(token_count, head_count, value_width), cumulative.reshape(token_count, head_count, key_width), totals, states)

def slot_positions(route_rows, expert_count, capacity):
    flattened = route_rows.reshape(-1)
    onehot = (flattened[:, None] == jnp.arange(expert_count, dtype=jnp.int32)[None, :]).astype(jnp.int32)
    before = jnp.cumsum(onehot, axis=0) - onehot
    slot_rank = lax.optimization_barrier(jnp.sum(before * onehot, axis=1))
    return (flattened * capacity + slot_rank).reshape(route_rows.shape).astype(jnp.int32)

def reference(mix_tokens, mix_gain, w_query, w_forget_fwd, w_forget_bwd, w_value, decay_floor, decay_shift, head_gain, w_out, moe_tokens, moe_gain, routes, route_logits, w_expert_gate, w_expert_up, w_expert_down):
    normed = rms_rows(mix_tokens, mix_gain).astype(jnp.bfloat16)

    def project(weight):
        return jnp.dot(normed, weight, preferred_element_type=jnp.float32).astype(jnp.bfloat16)
    queries = jax.nn.silu(project(w_query).astype(jnp.float32)).reshape(ROWS, HEADS, DK)
    values = project(w_value).astype(jnp.float32).reshape(ROWS, HEADS, DV)
    keys_fwd, forward_log_decay = decay_terms(project(w_forget_fwd), decay_floor, decay_shift, HEADS)
    keys_bwd, logs_bwd = decay_terms(project(w_forget_bwd), decay_floor, decay_shift, HEADS)
    out_fwd = sweep_blocks(queries, keys_fwd, values, forward_log_decay, 128)[0]
    out_bwd = sweep_blocks(jnp.flip(queries, 0), jnp.flip(keys_bwd, 0), jnp.flip(values, 0), jnp.flip(logs_bwd, 0), 128)[0]
    combined = out_fwd + jnp.flip(out_bwd, 0)
    readout = rms_rows(combined, head_gain).reshape(ROWS, HEADS * DV).astype(jnp.bfloat16)
    mixed_out = jnp.dot(readout, w_out, preferred_element_type=jnp.float32).astype(jnp.bfloat16)
    normed_moe = rms_rows(moe_tokens, moe_gain).astype(jnp.bfloat16)
    blocks = routes.reshape(N_EP, M_EP, TOPK)
    position = jax.vmap(functools.partial(slot_positions, expert_count=EXPERTS, capacity=CAP))(blocks)
    local_rows = jnp.arange(TOPK * M_EP, dtype=jnp.int32) // TOPK

    def slot_table(block_pos, source):
        filled = jnp.full((EXPERTS * CAP,), MROWS, jnp.int32)
        return filled.at[block_pos.reshape(-1)].set(source * M_EP + local_rows)
    tables = jax.vmap(slot_table)(position, jnp.arange(N_EP, dtype=jnp.int32))
    by_expert = tables.reshape(N_EP, EXPERTS, CAP).transpose(1, 0, 2).reshape(EXPERTS, N_EP * CAP)
    padded = jnp.concatenate([normed_moe, jnp.zeros((1, D), jnp.bfloat16)], axis=0)
    group_cols = FF // N_TP

    def expert_rows(expert_args):
        rows_index, gate_weight, up_weight, down_weight = expert_args
        row_data = padded[rows_index]
        gate_acts = jnp.dot(row_data, gate_weight, preferred_element_type=jnp.float32)
        up_acts = jnp.dot(row_data, up_weight, preferred_element_type=jnp.float32)
        hidden = (jax.nn.silu(gate_acts) * up_acts).astype(jnp.bfloat16)
        summed = jnp.zeros((row_data.shape[0], D), jnp.float32)
        for step_index in range(N_TP):
            partial_value = jnp.dot(hidden[:, step_index * group_cols:(step_index + 1) * group_cols], down_weight[step_index * group_cols:(step_index + 1) * group_cols], preferred_element_type=jnp.float32).astype(jnp.bfloat16)
            summed = summed + lax.optimization_barrier(partial_value).astype(jnp.float32)
        return summed.astype(jnp.bfloat16)
    results = lax.map(expert_rows, (by_expert, w_expert_gate, w_expert_up, w_expert_down))
    slot_of = position - blocks * CAP
    sources = jnp.arange(N_EP, dtype=jnp.int32)[:, None, None]
    flat_index = ((blocks * N_EP + sources) * CAP + slot_of).reshape(MROWS, TOPK)
    picked = results.reshape(EXPERTS * N_EP * CAP, D)[flat_index].astype(jnp.float32)
    weights = jax.nn.sigmoid(route_logits - jnp.flip(route_logits, 1))
    moe_out = lax.optimization_barrier(jnp.sum(picked * weights[:, :, None], axis=1)).astype(jnp.bfloat16)
    return (mixed_out, moe_out)
```

```python
import functools

import jax
import jax.numpy as jnp
from jax import lax
from jax.experimental import pallas as pl
from jax.experimental.pallas import tpu as pltpu
from jax.sharding import Mesh
from jax.sharding import PartitionSpec as P

DK = 128
DV = 128
BLK = 128
EP = ("z", "x")
TP = ("y", "c")
ALL = ("z", "x", "y", "c")
EPSILON = 1e-06
BF = jnp.bfloat16
F32 = jnp.float32
CHUNKS = ((0, 72),)
VMEM_LIMIT = 56 * 1024 * 1024


def params(*semantics):
    return pltpu.CompilerParams(
        dimension_semantics=semantics if semantics else None, vmem_limit_bytes=VMEM_LIMIT
    )


def dot(a, b):
    return jnp.dot(a, b, preferred_element_type=F32)


def dot_nt(a, b):
    return lax.dot_general(a, b, (((1,), (1,)), ((), ())), preferred_element_type=F32)


def dot_tn(a, b):
    return lax.dot_general(a, b, (((0,), (0,)), ((), ())), preferred_element_type=F32)


def rms_scale(floats):
    return lax.rsqrt(jnp.mean(floats * floats, axis=-1, keepdims=True) + EPSILON)


def dispatch_kernel(idx_ref, tok_ref, gain_ref, routes_ref, *outs, chunks, experts):
    half = tok_ref.shape[1] // 2
    rows = tok_ref.shape[0]
    scale = rms_scale(tok_ref[...].astype(F32))
    start = pl.multiple_of(idx_ref[0] * half, half)
    own = tok_ref[:, pl.ds(start, half)].astype(F32)
    normed = (own * scale * gain_ref[:, pl.ds(start, half)]).astype(BF)
    e0 = routes_ref[0:1, :]
    e1 = routes_ref[1:2, :]
    expert_iota = lax.broadcasted_iota(jnp.int32, (experts, rows), 0)
    oh0 = (expert_iota == e0).astype(F32)
    oh1 = (expert_iota == e1).astype(F32)
    earlier = (
        lax.broadcasted_iota(jnp.int32, (rows, rows), 0)
        < lax.broadcasted_iota(jnp.int32, (rows, rows), 1)
    ).astype(F32)
    before = dot((oh0 + oh1).astype(BF), earlier.astype(BF))
    slot0 = jnp.sum(oh0 * before, axis=0, keepdims=True).astype(jnp.int32)
    slot1 = jnp.sum(oh1 * (before + oh0), axis=0, keepdims=True).astype(jnp.int32)
    for out, (first, count) in zip(outs, chunks):
        total = experts * count

        def place(expert, slot):
            inside = (slot >= first) & (slot < first + count)
            return jnp.where(inside, expert * count + slot - first, -1)

        p0 = place(e0, slot0)
        p1 = place(e1, slot1)
        row_iota = lax.broadcasted_iota(jnp.int32, (total, rows), 0)
        chosen = ((row_iota == p0) | (row_iota == p1)).astype(F32).astype(BF)
        out[...] = dot(chosen, normed).astype(BF)


def dispatch(idx, tokens, gain, routes_t, experts):
    half = tokens.shape[1] // 2
    return pl.pallas_call(
        functools.partial(dispatch_kernel, chunks=CHUNKS, experts=experts),
        out_shape=tuple(jax.ShapeDtypeStruct((experts * n, half), BF) for _, n in CHUNKS),
        in_specs=[
            pl.BlockSpec(memory_space=pltpu.SMEM),
            pl.BlockSpec(memory_space=pltpu.VMEM),
            pl.BlockSpec(memory_space=pltpu.VMEM),
            pl.BlockSpec(memory_space=pltpu.VMEM),
        ],
        out_specs=tuple(pl.BlockSpec(memory_space=pltpu.VMEM) for _ in CHUNKS),
        compiler_params=params(),
        name="dispatch",
    )(idx, tokens, gain, routes_t)


def tri_sum(tri, g):
    high = g.astype(BF)
    low = (g - high.astype(F32)).astype(BF)
    return dot(tri, high) + dot(tri, low)


def local_kernel(
    x_ref,
    gain_ref,
    wq_ref,
    wf_ref,
    wb_ref,
    wv_ref,
    floor_ref,
    shift_ref,
    o_ref,
    qf_ref,
    qb_ref,
    msg_ref,
    q_s,
    v_s,
    kb_s,
    gb_s,
    st_s,
    off_s,
    *,
    steps,
    rows,
    heads,
):
    step = pl.program_id(0)
    width = heads * DK

    @pl.when(step == 0)
    def _():
        st_s[...] = jnp.zeros_like(st_s)
        off_s[...] = jnp.zeros_like(off_s)

    x = x_ref[...].astype(F32)
    normed = (x * rms_scale(x) * gain_ref[...]).astype(BF)

    def project(w_ref):
        return dot(normed, w_ref[...]).astype(BF)

    q_pre = project(wq_ref).astype(F32)
    queries = q_pre * jax.nn.sigmoid(q_pre)
    values = project(wv_ref)
    shift = shift_ref[...]
    shift_wide = jnp.concatenate(
        [jnp.broadcast_to(shift[:, h : h + 1], (rows, DK)) for h in range(heads)], axis=1
    )
    room = 1.0 - floor_ref[...]

    def decay(w_ref):
        keys = room * (1.0 - jax.nn.sigmoid(project(w_ref).astype(F32)))
        return keys, jnp.log1p(-keys) + shift_wide

    keys_f, logs_f = decay(wf_ref)
    keys_b, logs_b = decay(wb_ref)
    base = pl.multiple_of(step * rows, rows)
    q_s[pl.ds(base, rows), :] = queries
    v_s[pl.ds(base, rows), :] = values
    kb_s[pl.ds(base, rows), :] = keys_b
    gb_s[pl.ds(base, rows), :] = logs_b

    row_iota = lax.broadcasted_iota(jnp.int32, (BLK, BLK), 0)
    col_iota = lax.broadcasted_iota(jnp.int32, (BLK, BLK), 1)
    lower = row_iota >= col_iota
    upper = row_iota <= col_iota
    lower_one = lower.astype(F32).astype(BF)
    upper_one = upper.astype(F32).astype(BF)

    def block(q, k, v, g, tri_one, mask, end_row, states, offset):
        run = tri_sum(tri_one, g)
        end = run[end_row : end_row + 1, :]
        grown = q * jnp.exp(run)
        grown_b = grown.astype(BF)
        shrunk = (k * jnp.exp(-run)).astype(BF)
        closing = (k * jnp.exp(end - run)).astype(BF)
        kept = jnp.exp(end)
        result = []
        new_states = []
        for h in range(heads):
            lanes = slice(h * DK, (h + 1) * DK)
            scores = jnp.where(mask, dot_nt(grown_b[:, lanes], shrunk[:, lanes]), 0.0).astype(BF)
            st = states[h]
            result.append(
                dot(scores, v[:, lanes]) + dot_nt(grown_b[:, lanes], st.astype(BF))
            )
            new_states.append(st * kept[:, lanes] + dot_tn(v[:, lanes], closing[:, lanes]))
        carried = (grown * jnp.exp(offset)).astype(BF)
        return jnp.concatenate(result, axis=1), new_states, carried, offset + end

    def write_message(first, states, total):
        kept = jnp.exp(total)
        high = kept.astype(BF)
        low = (kept - high.astype(F32)).astype(BF)
        for h in range(heads):
            lanes = slice(h * DK, (h + 1) * DK)
            tail = jnp.concatenate(
                [high[:, lanes], low[:, lanes], jnp.zeros((6, DK), BF)], axis=0
            )
            for part in range(4):
                msg_ref[first + h * 4 + part, 0:32, :] = states[h][
                    part * 32 : (part + 1) * 32, :
                ].astype(BF)
                msg_ref[first + h * 4 + part, 32:40, :] = tail

    states = [st_s[h] for h in range(heads)]
    offset = off_s[...]
    for b in range(rows // BLK):
        rs = slice(b * BLK, (b + 1) * BLK)
        result, states, carried, offset = block(
            queries[rs], keys_f[rs], values[rs], logs_f[rs], lower_one, lower, BLK - 1, states, offset
        )
        at = pl.multiple_of(base + b * BLK, BLK)
        o_ref[pl.ds(at, BLK), :] = result
        qf_ref[pl.ds(at, BLK), :] = carried
    for h in range(heads):
        st_s[h] = states[h]
    off_s[...] = offset

    @pl.when(step == steps - 1)
    def _():
        write_message(0, states, offset)
        back = [jnp.zeros((DV, DK), F32) for _ in range(heads)]
        total = jnp.zeros((1, width), F32)
        for b in reversed(range(steps * rows // BLK)):
            rs = slice(b * BLK, (b + 1) * BLK)
            result, back, carried, total = block(
                q_s[rs, :], kb_s[rs, :], v_s[rs, :], gb_s[rs, :], upper_one, upper, 0, back, total
            )
            o_ref[rs, :] = o_ref[rs, :] + result
            qb_ref[rs, :] = carried
        write_message(4 * heads, back, total)


def local_sweeps(tokens, gain, wq, wf, wb, wv, floor, shift):
    seg, model = tokens.shape
    width = wq.shape[1]
    heads = width // DK
    rows = 256
    steps = seg // rows
    whole = lambda shape: pl.BlockSpec(shape, lambda i: tuple(0 for _ in shape))
    return pl.pallas_call(
        functools.partial(local_kernel, steps=steps, rows=rows, heads=heads),
        grid=(steps,),
        out_shape=(
            jax.ShapeDtypeStruct((seg, width), F32),
            jax.ShapeDtypeStruct((seg, width), BF),
            jax.ShapeDtypeStruct((seg, width), BF),
            jax.ShapeDtypeStruct((8 * heads, 40, DK), BF),
        ),
        in_specs=[
            pl.BlockSpec((rows, model), lambda i: (i, 0)),
            whole((1, model)),
            whole((model, width)),
            whole((model, width)),
            whole((model, width)),
            whole((model, width)),
            whole((1, width)),
            pl.BlockSpec((rows, heads), lambda i: (i, 0)),
        ],
        out_specs=(
            whole((seg, width)),
            whole((seg, width)),
            whole((seg, width)),
            whole((8 * heads, 40, DK)),
        ),
        scratch_shapes=[
            pltpu.VMEM((seg, width), F32),
            pltpu.VMEM((seg, width), BF),
            pltpu.VMEM((seg, width), F32),
            pltpu.VMEM((seg, width), F32),
            pltpu.VMEM((heads, DV, DK), F32),
            pltpu.VMEM((1, width), F32),
        ],
        compiler_params=params("arbitrary"),
        name="local_sweeps",
    )(tokens, gain, wq, wf, wb, wv, floor, shift)


def scan_kernel(idx_ref, msg_ref, out_ref):
    count = msg_ref.shape[0]
    backward = idx_ref[2] >= count // 2
    state = jnp.zeros((32, DK), F32)
    for i in range(count):
        at = jnp.where(backward, count - 1 - i, i)
        out_ref[at] = state.astype(BF)
        block = msg_ref[at].astype(F32)
        kept = block[32:33, :] + block[33:34, :]
        state = state * kept + block[0:32, :]


def scan_states(idx, message):
    return pl.pallas_call(
        scan_kernel,
        out_shape=jax.ShapeDtypeStruct((message.shape[0], 32, DK), BF),
        in_specs=[
            pl.BlockSpec(memory_space=pltpu.SMEM),
            pl.BlockSpec(memory_space=pltpu.VMEM),
        ],
        out_specs=pl.BlockSpec(memory_space=pltpu.VMEM),
        compiler_params=params(),
        name="scan_states",
    )(idx, message)


def finish_kernel(o_ref, qf_ref, qb_ref, states_ref, gain_ref, out_ref, *, heads):
    for h in range(heads):
        lanes = slice(h * DK, (h + 1) * DK)
        ahead = states_ref[h * DV : (h + 1) * DV, :]
        behind = states_ref[(heads + h) * DV : (heads + h + 1) * DV, :]
        o = (
            o_ref[:, lanes]
            + dot_nt(qf_ref[:, lanes], ahead)
            + dot_nt(qb_ref[:, lanes], behind)
        )
        out_ref[:, lanes] = (o * rms_scale(o) * gain_ref[...]).astype(BF)


def finish(o, qf, qb, states, gain):
    seg, width = o.shape
    rows = 256
    tile = pl.BlockSpec((rows, width), lambda i: (i, 0))
    return pl.pallas_call(
        functools.partial(finish_kernel, heads=width // DK),
        grid=(seg // rows,),
        out_shape=jax.ShapeDtypeStruct((seg, width), BF),
        in_specs=[
            tile,
            tile,
            tile,
            pl.BlockSpec(states.shape, lambda i: (0, 0)),
            pl.BlockSpec((1, DV), lambda i: (0, 0)),
        ],
        out_specs=tile,
        compiler_params=params("arbitrary"),
        name="finish",
    )(o, qf, qb, states, gain)


def project_kernel(r_ref, w_ref, out_ref):
    groups, _, width = r_ref.shape
    rows = jnp.concatenate([r_ref[g] for g in range(groups)], axis=1)
    out_ref[...] = dot(rows, w_ref[...]).astype(BF)


def project_out(regrouped, w_out):
    groups, rows, width = regrouped.shape
    model = w_out.shape[1]
    cols = 512
    return pl.pallas_call(
        project_kernel,
        grid=(model // cols,),
        out_shape=jax.ShapeDtypeStruct((rows, model), BF),
        in_specs=[
            pl.BlockSpec((groups, rows, width), lambda j: (0, 0, 0)),
            pl.BlockSpec((groups * width, cols), lambda j: (0, j)),
        ],
        out_specs=pl.BlockSpec((rows, cols), lambda j: (0, j)),
        compiler_params=params("arbitrary"),
        name="project_out",
    )(regrouped, w_out)


def hidden_kernel(idx_ref, own_ref, other_ref, wg_ref, wu_ref, wd_ref, h_ref, part_ref, *, groups):
    core = idx_ref[0]
    half = own_ref.shape[1]
    cols = part_ref.shape[2]
    mine = pl.ds(pl.multiple_of(core * half, half), half)
    theirs = pl.ds(pl.multiple_of((1 - core) * half, half), half)
    own = own_ref[...]
    other = other_ref[...]
    gate = dot(own, wg_ref[mine, :]) + dot(other, wg_ref[theirs, :])
    up = dot(own, wu_ref[mine, :]) + dot(other, wu_ref[theirs, :])
    hidden = (gate * jax.nn.sigmoid(gate) * up).astype(BF)
    h_ref[...] = hidden
    for g in range(groups):
        start = pl.multiple_of((2 * g + 1 - core) * cols, cols)
        part_ref[g] = dot(hidden, wd_ref[:, pl.ds(start, cols)]).astype(BF)


def expert_hidden(idx, own, other, wg, wu, wd, groups, row_block):
    rows, half = own.shape
    ff = wg.shape[1]
    model = wd.shape[1]
    cols = model // (2 * groups)
    whole = lambda shape: pl.BlockSpec(shape, lambda i, s: tuple(0 for _ in shape))
    return pl.pallas_call(
        functools.partial(hidden_kernel, groups=groups),
        grid_spec=pltpu.PrefetchScalarGridSpec(
            num_scalar_prefetch=1,
            grid=(rows // row_block,),
            in_specs=[
                pl.BlockSpec((row_block, half), lambda i, s: (i, 0)),
                pl.BlockSpec((row_block, half), lambda i, s: (i, 0)),
                whole(wg.shape),
                whole(wu.shape),
                whole(wd.shape),
            ],
            out_specs=(
                pl.BlockSpec((row_block, ff), lambda i, s: (i, 0)),
                pl.BlockSpec((groups, row_block, cols), lambda i, s: (0, i, 0)),
            ),
        ),
        out_shape=(
            jax.ShapeDtypeStruct((rows, ff), BF),
            jax.ShapeDtypeStruct((groups, rows, cols), BF),
        ),
        compiler_params=params("arbitrary"),
        name="expert_hidden",
    )(idx, own, other, wg, wu, wd)


def down_kernel(idx_ref, h_ref, wd_ref, got_ref, out_ref):
    mine = dot(h_ref[...], wd_ref[...]).astype(BF)
    out_ref[0] = (mine.astype(F32) + got_ref[0].astype(F32)).astype(BF)


def expert_down(idx, hidden, wd, received, groups, row_block):
    rows, ff = hidden.shape
    cols = received.shape[2]
    block = lambda d, s: (s[1] + d) % groups
    return pl.pallas_call(
        down_kernel,
        grid_spec=pltpu.PrefetchScalarGridSpec(
            num_scalar_prefetch=1,
            grid=(groups,),
            in_specs=[
                pl.BlockSpec((rows, ff), lambda d, s: (0, 0)),
                pl.BlockSpec((ff, cols), lambda d, s: (0, 2 * block(d, s) + s[0])),
                pl.BlockSpec((1, rows, cols), lambda d, s: (block(d, s), 0, 0)),
            ],
            out_specs=pl.BlockSpec((1, rows, cols), lambda d, s: (d, 0, 0)),
        ),
        out_shape=jax.ShapeDtypeStruct((groups, rows, cols), BF),
        compiler_params=params("arbitrary"),
        name="expert_down",
    )(idx, hidden, wd, received)


def combine_kernel(routes_ref, logits_ref, *refs, chunks, experts):
    returned, out_ref = refs[:-1], refs[-1]
    rows = routes_ref.shape[0]
    expert_iota = lax.broadcasted_iota(jnp.int32, (rows, experts), 1)
    e0 = routes_ref[:, 0:1]
    e1 = routes_ref[:, 1:2]
    oh0 = (expert_iota == e0).astype(F32)
    oh1 = (expert_iota == e1).astype(F32)
    earlier = (
        lax.broadcasted_iota(jnp.int32, (rows, rows), 1)
        < lax.broadcasted_iota(jnp.int32, (rows, rows), 0)
    ).astype(F32)
    before = dot(earlier.astype(BF), (oh0 + oh1).astype(BF))
    slot0 = jnp.sum(oh0 * before, axis=1, keepdims=True).astype(jnp.int32)
    slot1 = jnp.sum(oh1 * (before + oh0), axis=1, keepdims=True).astype(jnp.int32)
    logits = logits_ref[...]
    gap = logits[:, 0:1] - logits[:, 1:2]

    def picked(expert, slot):
        total = 0.0
        for ref, (first, count) in zip(returned, chunks):
            inside = (slot >= first) & (slot < first + count)
            place = jnp.where(inside, expert * count + slot - first, -1)
            lane_iota = lax.broadcasted_iota(jnp.int32, (rows, experts * count), 1)
            chosen = (lane_iota == place).astype(F32).astype(BF)
            total = total + dot(chosen, ref[...])
        return total

    out_ref[...] = (
        picked(e0, slot0) * jax.nn.sigmoid(gap) + picked(e1, slot1) * jax.nn.sigmoid(-gap)
    ).astype(BF)


def combine(routes, logits, returned, experts):
    rows = routes.shape[0]
    cols = returned[0].shape[1]
    return pl.pallas_call(
        functools.partial(combine_kernel, chunks=CHUNKS, experts=experts),
        out_shape=jax.ShapeDtypeStruct((rows, cols), BF),
        in_specs=[pl.BlockSpec(memory_space=pltpu.VMEM) for _ in range(2 + len(returned))],
        out_specs=pl.BlockSpec(memory_space=pltpu.VMEM),
        compiler_params=params(),
        name="combine",
    )(routes, logits, *returned)


def ring(count, shift):
    return [(i, (i + shift) % count) for i in range(count)]


def body(
    mix_tokens,
    mix_gain,
    w_query,
    w_forget_fwd,
    w_forget_bwd,
    w_value,
    decay_floor,
    decay_shift,
    head_gain,
    w_out,
    moe_tokens,
    moe_gain,
    routes,
    route_logits,
    w_expert_gate,
    w_expert_up,
    w_expert_down,
):
    experts = lax.axis_size(EP)
    groups = lax.axis_size("y")
    core, chip = lax.axis_index("c"), lax.axis_index("y")
    idx = jnp.stack([core, chip, lax.axis_index(EP)]).astype(jnp.int32)
    swap = [(0, 1), (1, 0)]
    wg, wu, wd = w_expert_gate[0], w_expert_up[0], w_expert_down[0]

    outgoing = dispatch(idx, moe_tokens, moe_gain[None], routes.T, experts)
    arrived = []
    for rows, (_, count) in zip(outgoing, CHUNKS):
        shaped = rows.reshape(experts, count, rows.shape[1])
        got = lax.all_to_all(shaped, EP, split_axis=0, concat_axis=0, tiled=True)
        arrived.append(got.reshape(rows.shape))

    o, qf, qb, message = local_sweeps(
        mix_tokens,
        mix_gain[None],
        w_query,
        w_forget_fwd,
        w_forget_bwd,
        w_value,
        decay_floor[None],
        decay_shift,
    )
    summaries = lax.all_to_all(message, EP, split_axis=0, concat_axis=0, tiled=True)
    incoming = scan_states(idx, summaries)
    incoming = lax.all_to_all(incoming, EP, split_axis=0, concat_axis=0, tiled=True)

    returned = []
    for own, (_, count) in zip(arrived, CHUNKS):
        other = lax.ppermute(own, "c", swap)
        block = own.shape[0] // max(1, own.shape[0] // 320)
        hidden, for_partner = expert_hidden(idx, own, other, wg, wu, wd, groups, block)
        received = lax.ppermute(for_partner, "c", swap)
        pair = expert_down(idx, hidden, wd, received, groups, block)
        parts = [pair[0]] + [lax.ppermute(pair[d], "y", ring(groups, d)) for d in range(1, groups)]
        summed = sum(part.astype(F32) for part in parts).astype(BF)
        shaped = summed.reshape(experts, count, summed.shape[1])
        back = lax.all_to_all(shaped, EP, split_axis=0, concat_axis=0, tiled=True)
        returned.append(back.reshape(summed.shape))

    readout = finish(o, qf, qb, incoming.reshape(-1, DK), head_gain[None])
    tp_size = lax.axis_size(TP)
    shaped = readout.reshape(tp_size, -1, readout.shape[1])
    regrouped = lax.all_to_all(shaped, TP, split_axis=0, concat_axis=0, tiled=True)
    mixed_out = project_out(regrouped, w_out)
    moe_out = combine(routes, route_logits, returned, experts)
    return (mixed_out, moe_out)


def solution(mesh):
    finer = Mesh(mesh.devices.reshape(4, 4, 4, 2), ALL)
    return jax.shard_map(
        body,
        mesh=finer,
        in_specs=(
            P(EP, None),
            P(),
            P(None, TP),
            P(None, TP),
            P(None, TP),
            P(None, TP),
            P(TP),
            P(EP, TP),
            P(),
            P(),
            P(EP, None),
            P(),
            P(EP, None),
            P(EP, None),
            P(EP, None, TP),
            P(EP, None, TP),
            P(EP, TP, None),
        ),
        out_specs=(P(ALL, None), P(EP, TP)),
        check_vma=False,
    )
```

```python
import functools

import jax
import jax.numpy as jnp
from jax import lax
from jax.experimental import pallas as pl
from jax.experimental.pallas import tpu as pltpu
from jax.sharding import Mesh
from jax.sharding import PartitionSpec as P

DK = 128
DV = 128
BLK = 128
EP = ("z", "x")
TP = ("y", "c")
ALL = ("z", "x", "y", "c")
EPSILON = 1e-06
BF = jnp.bfloat16
F32 = jnp.float32
CHUNKS = ((0, 72),)
COST_UNIT = 250e6


def params(mib, *semantics):
    return pltpu.CompilerParams(
        dimension_semantics=semantics if semantics else None, vmem_limit_bytes=mib * 1024 * 1024
    )


def cost(micros):
    return pl.CostEstimate(flops=int(micros * COST_UNIT), transcendentals=0, bytes_accessed=0)


def after(kernel, at, deps):
    def run(*refs):
        kernel(*refs[:at], *refs[at + len(deps) :])

    return run


def any_specs(deps):
    return [pl.BlockSpec(memory_space=pl.ANY) for _ in deps]


def dot(a, b):
    return jnp.dot(a, b, preferred_element_type=F32)


def dot_nt(a, b):
    return lax.dot_general(a, b, (((1,), (1,)), ((), ())), preferred_element_type=F32)


def dot_tn(a, b):
    return lax.dot_general(a, b, (((0,), (0,)), ((), ())), preferred_element_type=F32)


def rms_scale(floats):
    return lax.rsqrt(jnp.mean(floats * floats, axis=-1, keepdims=True) + EPSILON)


def dispatch_kernel(idx_ref, tok_ref, gain_ref, routes_ref, *outs, chunks, experts):
    half = tok_ref.shape[1] // 2
    rows = tok_ref.shape[0]
    scale = rms_scale(tok_ref[...].astype(F32))
    start = pl.multiple_of(idx_ref[0] * half, half)
    own = tok_ref[:, pl.ds(start, half)].astype(F32)
    normed = (own * scale * gain_ref[:, pl.ds(start, half)]).astype(BF)
    e0 = routes_ref[0:1, :]
    e1 = routes_ref[1:2, :]
    expert_iota = lax.broadcasted_iota(jnp.int32, (experts, rows), 0)
    oh0 = (expert_iota == e0).astype(F32)
    oh1 = (expert_iota == e1).astype(F32)
    earlier = (
        lax.broadcasted_iota(jnp.int32, (rows, rows), 0)
        < lax.broadcasted_iota(jnp.int32, (rows, rows), 1)
    ).astype(F32)
    before = dot((oh0 + oh1).astype(BF), earlier.astype(BF))
    slot0 = jnp.sum(oh0 * before, axis=0, keepdims=True).astype(jnp.int32)
    slot1 = jnp.sum(oh1 * (before + oh0), axis=0, keepdims=True).astype(jnp.int32)
    for out, (first, count) in zip(outs, chunks):
        total = experts * count

        def place(expert, slot):
            inside = (slot >= first) & (slot < first + count)
            return jnp.where(inside, expert * count + slot - first, -1)

        p0 = place(e0, slot0)
        p1 = place(e1, slot1)
        row_iota = lax.broadcasted_iota(jnp.int32, (total, rows), 0)
        chosen = ((row_iota == p0) | (row_iota == p1)).astype(F32).astype(BF)
        out[...] = dot(chosen, normed).astype(BF)


def dispatch(idx, tokens, gain, routes_t, experts):
    half = tokens.shape[1] // 2
    return pl.pallas_call(
        functools.partial(dispatch_kernel, chunks=CHUNKS, experts=experts),
        out_shape=tuple(jax.ShapeDtypeStruct((experts * n, half), BF) for _, n in CHUNKS),
        in_specs=[
            pl.BlockSpec(memory_space=pltpu.SMEM),
            pl.BlockSpec(memory_space=pltpu.VMEM),
            pl.BlockSpec(memory_space=pltpu.VMEM),
            pl.BlockSpec(memory_space=pltpu.VMEM),
        ],
        out_specs=tuple(pl.BlockSpec(memory_space=pltpu.VMEM) for _ in CHUNKS),
        compiler_params=params(16),
        cost_estimate=cost(5),
        name="dispatch",
    )(idx, tokens, gain, routes_t)


def tri_sum(tri, g):
    high = g.astype(BF)
    low = (g - high.astype(F32)).astype(BF)
    return dot(tri, high) + dot(tri, low)


def local_kernel(
    idx_ref,
    x_ref,
    gain_ref,
    wq_ref,
    wf_ref,
    wb_ref,
    wv_ref,
    floor_ref,
    shift_ref,
    o_ref,
    qf_ref,
    qb_ref,
    msg_ref,
    q_s,
    v_s,
    kb_s,
    gb_s,
    st_s,
    off_s,
    kept_s,
    *,
    steps,
    rows,
    heads,
):
    step = pl.program_id(0)
    width = heads * DK

    @pl.when(step == 0)
    def _():
        st_s[...] = jnp.zeros_like(st_s)
        off_s[...] = jnp.zeros_like(off_s)
        kept_s[...] = jnp.zeros_like(kept_s)

    x = x_ref[...].astype(F32)
    normed = (x * rms_scale(x) * gain_ref[...]).astype(BF)

    def project(w_ref):
        return dot(normed, w_ref[...]).astype(BF)

    q_pre = project(wq_ref).astype(F32)
    queries = q_pre * jax.nn.sigmoid(q_pre)
    values = project(wv_ref)
    shift = shift_ref[...]
    shift_wide = jnp.concatenate(
        [jnp.broadcast_to(shift[:, h : h + 1], (rows, DK)) for h in range(heads)], axis=1
    )
    room = 1.0 - floor_ref[...]

    def decay(w_ref):
        keys = room * (1.0 - jax.nn.sigmoid(project(w_ref).astype(F32)))
        return keys, jnp.log1p(-keys) + shift_wide

    keys_f, logs_f = decay(wf_ref)
    keys_b, logs_b = decay(wb_ref)
    base = pl.multiple_of(step * rows, rows)
    q_s[pl.ds(base, rows), :] = queries
    v_s[pl.ds(base, rows), :] = values
    kb_s[pl.ds(base, rows), :] = keys_b
    gb_s[pl.ds(base, rows), :] = logs_b

    row_iota = lax.broadcasted_iota(jnp.int32, (BLK, BLK), 0)
    col_iota = lax.broadcasted_iota(jnp.int32, (BLK, BLK), 1)
    lower = row_iota >= col_iota
    upper = row_iota <= col_iota
    lower_one = lower.astype(F32).astype(BF)
    upper_one = upper.astype(F32).astype(BF)

    def block(q, k, v, g, tri_one, mask, end_row, states, offset):
        run = tri_sum(tri_one, g)
        end = run[end_row : end_row + 1, :]
        grown = q * jnp.exp(run)
        grown_b = grown.astype(BF)
        shrunk = (k * jnp.exp(-run)).astype(BF)
        closing = (k * jnp.exp(end - run)).astype(BF)
        kept = jnp.exp(end)
        result = []
        new_states = []
        for h in range(heads):
            lanes = slice(h * DK, (h + 1) * DK)
            scores = jnp.where(mask, dot_nt(grown_b[:, lanes], shrunk[:, lanes]), 0.0).astype(BF)
            st = states[h]
            result.append(
                dot(scores, v[:, lanes]) + dot_nt(grown_b[:, lanes], st.astype(BF))
            )
            new_states.append(st * kept[:, lanes] + dot_tn(v[:, lanes], closing[:, lanes]))
        carried = (grown * jnp.exp(offset)).astype(BF)
        return jnp.concatenate(result, axis=1), new_states, carried, offset + end

    def write_message(way, states, total):
        kept = jnp.exp(total)
        high = kept.astype(BF).astype(F32)
        for h in range(heads):
            lanes = slice(h * DK, (h + 1) * DK)
            kept_s[h : h + 1, :] = high[:, lanes]
            kept_s[heads + h : heads + h + 1, :] = (kept - high)[:, lanes]
        whole = jnp.concatenate(list(states) + [kept_s[...]], axis=0).astype(BF)

        def write(target, _):
            msg_ref[target] = whole
            return 0

        here = idx_ref[2]
        if way == 0:
            lax.fori_loop(here, msg_ref.shape[0], write, 0)
        else:
            lax.fori_loop(0, here, write, 0)

    states = [st_s[h] for h in range(heads)]
    offset = off_s[...]
    for b in range(rows // BLK):
        rs = slice(b * BLK, (b + 1) * BLK)
        result, states, carried, offset = block(
            queries[rs], keys_f[rs], values[rs], logs_f[rs], lower_one, lower, BLK - 1, states, offset
        )
        at = pl.multiple_of(base + b * BLK, BLK)
        o_ref[pl.ds(at, BLK), :] = result
        qf_ref[pl.ds(at, BLK), :] = carried
    for h in range(heads):
        st_s[h] = states[h]
    off_s[...] = offset

    @pl.when(step == steps - 1)
    def _():
        write_message(0, states, offset)
        back = [jnp.zeros((DV, DK), F32) for _ in range(heads)]
        total = jnp.zeros((1, width), F32)
        for b in reversed(range(steps * rows // BLK)):
            rs = slice(b * BLK, (b + 1) * BLK)
            result, back, carried, total = block(
                q_s[rs, :], kb_s[rs, :], v_s[rs, :], gb_s[rs, :], upper_one, upper, 0, back, total
            )
            o_ref[rs, :] = o_ref[rs, :] + result
            qb_ref[rs, :] = carried
        write_message(1, back, total)


def local_sweeps(idx, tokens, gain, wq, wf, wb, wv, floor, shift, segments, deps=()):
    seg, model = tokens.shape
    width = wq.shape[1]
    heads = width // DK
    rows = 256
    steps = seg // rows
    whole = lambda shape: pl.BlockSpec(shape, lambda i: tuple(0 for _ in shape))
    return pl.pallas_call(
        after(functools.partial(local_kernel, steps=steps, rows=rows, heads=heads), 9, deps),
        grid=(steps,),
        out_shape=(
            jax.ShapeDtypeStruct((seg, width), F32),
            jax.ShapeDtypeStruct((seg, width), BF),
            jax.ShapeDtypeStruct((seg, width), BF),
            jax.ShapeDtypeStruct((segments, heads * DV + 8, DK), BF),
        ),
        in_specs=[
            pl.BlockSpec(memory_space=pltpu.SMEM),
            pl.BlockSpec((rows, model), lambda i: (i, 0)),
            whole((1, model)),
            whole((model, width)),
            whole((model, width)),
            whole((model, width)),
            whole((model, width)),
            whole((1, width)),
            pl.BlockSpec((rows, heads), lambda i: (i, 0)),
            *any_specs(deps),
        ],
        out_specs=(
            whole((seg, width)),
            whole((seg, width)),
            whole((seg, width)),
            whole((segments, heads * DV + 8, DK)),
        ),
        scratch_shapes=[
            pltpu.VMEM((seg, width), F32),
            pltpu.VMEM((seg, width), BF),
            pltpu.VMEM((seg, width), F32),
            pltpu.VMEM((seg, width), F32),
            pltpu.VMEM((heads, DV, DK), F32),
            pltpu.VMEM((1, width), F32),
            pltpu.VMEM((8, DK), F32),
        ],
        compiler_params=params(28, "arbitrary"),
        cost_estimate=cost(17),
        name="local_sweeps",
    )(idx, tokens, gain, wq, wf, wb, wv, floor, shift, *deps)


def finish_kernel(idx_ref, *refs, heads):
    line_ref, gain_ref, *outs, states_ref = refs[6:]
    here = idx_ref[2]
    count = line_ref.shape[0]

    @pl.when(pl.program_id(0) == 0)
    def _():
        zeros = tuple(jnp.zeros((DV, DK), F32) for _ in range(heads))

        def join(source, states):
            new = []
            for h, state in enumerate(states):
                tail = line_ref[source, heads * DV :, :].astype(F32)
                kept = tail[h : h + 1, :] + tail[heads + h : heads + h + 1, :]
                new.append(
                    state * kept + line_ref[source, h * DV : (h + 1) * DV, :].astype(F32)
                )
            return tuple(new)

        ahead = lax.fori_loop(0, here, join, zeros)
        behind = lax.fori_loop(0, count - 1 - here, lambda i, st: join(count - 1 - i, st), zeros)
        for p, state in enumerate(ahead + behind):
            states_ref[p * DV : (p + 1) * DV, :] = state.astype(BF)

    for (o_ref, qf_ref, qb_ref), out_ref in zip((refs[0:3], refs[3:6]), outs):
        for h in range(heads):
            lanes = slice(h * DK, (h + 1) * DK)
            ahead = states_ref[h * DV : (h + 1) * DV, :]
            behind = states_ref[(heads + h) * DV : (heads + h + 1) * DV, :]
            o = (
                o_ref[:, lanes]
                + dot_nt(qf_ref[:, lanes], ahead)
                + dot_nt(qb_ref[:, lanes], behind)
            )
            out_ref[0, :, lanes] = (o * rms_scale(o) * gain_ref[...]).astype(BF)


def finish(idx, o, qf, qb, line, gain, groups, deps=()):
    seg, width = o.shape
    rows = seg // (2 * groups)

    def tile(other):
        return pl.BlockSpec(
            (rows, width), lambda d, s: (2 * ((s[1] + d) % groups) + jnp.bitwise_xor(s[0], other), 0)
        )

    out = pl.BlockSpec((1, rows, width), lambda d, s: (d, 0, 0))
    shape = jax.ShapeDtypeStruct((groups, rows, width), BF)
    return pl.pallas_call(
        after(functools.partial(finish_kernel, heads=width // DK), 9, deps),
        grid_spec=pltpu.PrefetchScalarGridSpec(
            num_scalar_prefetch=1,
            grid=(groups,),
            in_specs=[
                *(tile(other) for other in (0, 0, 0, 1, 1, 1)),
                pl.BlockSpec(line.shape, lambda d, s: (0, 0, 0)),
                pl.BlockSpec(gain.shape, lambda d, s: (0, 0)),
                *any_specs(deps),
            ],
            out_specs=(out, out),
            scratch_shapes=[pltpu.VMEM((2 * width, DK), BF)],
        ),
        out_shape=(shape, shape),
        compiler_params=params(12, "arbitrary"),
        cost_estimate=cost(4),
        name="finish",
    )(idx, o, qf, qb, o, qf, qb, line, gain, *deps)


def combine_kernel(routes_ref, logits_ref, *refs, chunks, experts):
    returned, out_ref = refs[:-1], refs[-1]
    rows = routes_ref.shape[0]
    expert_iota = lax.broadcasted_iota(jnp.int32, (rows, experts), 1)
    e0 = routes_ref[:, 0:1]
    e1 = routes_ref[:, 1:2]
    oh0 = (expert_iota == e0).astype(F32)
    oh1 = (expert_iota == e1).astype(F32)
    earlier = (
        lax.broadcasted_iota(jnp.int32, (rows, rows), 1)
        < lax.broadcasted_iota(jnp.int32, (rows, rows), 0)
    ).astype(F32)
    before = dot(earlier.astype(BF), (oh0 + oh1).astype(BF))
    slot0 = jnp.sum(oh0 * before, axis=1, keepdims=True).astype(jnp.int32)
    slot1 = jnp.sum(oh1 * (before + oh0), axis=1, keepdims=True).astype(jnp.int32)
    logits = logits_ref[...]
    gap = logits[:, 0:1] - logits[:, 1:2]

    def picked(expert, slot):
        total = 0.0
        for result, (first, count) in zip(returned, chunks):
            inside = (slot >= first) & (slot < first + count)
            place = jnp.where(inside, expert * count + slot - first, -1)
            lane_iota = lax.broadcasted_iota(jnp.int32, (rows, experts * count), 1)
            chosen = (lane_iota == place).astype(F32).astype(BF)
            total = total + dot(chosen, result[...])
        return total

    out_ref[...] = (
        picked(e0, slot0) * jax.nn.sigmoid(gap) + picked(e1, slot1) * jax.nn.sigmoid(-gap)
    ).astype(BF)


def combine(routes, logits, returned, experts):
    rows = routes.shape[0]
    cols = returned[0].shape[1]
    return pl.pallas_call(
        functools.partial(combine_kernel, chunks=CHUNKS, experts=experts),
        out_shape=jax.ShapeDtypeStruct((rows, cols), BF),
        in_specs=[pl.BlockSpec(memory_space=pltpu.VMEM) for _ in range(2 + len(returned))],
        out_specs=pl.BlockSpec(memory_space=pltpu.VMEM),
        compiler_params=params(12),
        cost_estimate=cost(4),
        name="combine",
    )(routes, logits, *returned)


def ring(count, shift):
    return [(i, (i + shift) % count) for i in range(count)]


def body(
    mix_tokens,
    mix_gain,
    w_query,
    w_forget_fwd,
    w_forget_bwd,
    w_value,
    decay_floor,
    decay_shift,
    head_gain,
    w_out,
    moe_tokens,
    moe_gain,
    routes,
    route_logits,
    w_expert_gate,
    w_expert_up,
    w_expert_down,
):
    experts = lax.axis_size(EP)
    groups = lax.axis_size("y")
    core, chip = lax.axis_index("c"), lax.axis_index("y")
    idx = jnp.stack([core, chip, lax.axis_index(EP)]).astype(jnp.int32)
    swap = [(0, 1), (1, 0)]
    wg, wu, wd = w_expert_gate[0], w_expert_up[0], w_expert_down[0]

    outgoing = dispatch(idx, moe_tokens, moe_gain[None], routes.T, experts)
    o, qf, qb, message = local_sweeps(
        idx,
        mix_tokens,
        mix_gain[None],
        w_query,
        w_forget_fwd,
        w_forget_bwd,
        w_value,
        decay_floor[None],
        decay_shift,
        experts,
        deps=outgoing,
    )
    part = wd.shape[1] // (2 * groups)

    def by_core(which):
        return jnp.concatenate(
            [
                lax.dynamic_slice_in_dim(wd, (2 * g + which) * part, part, axis=1)
                for g in range(groups)
            ],
            axis=1,
        )

    def rolled(weight, shares, order):
        rows = weight.shape[0] // shares
        return jnp.concatenate(
            [lax.dynamic_slice_in_dim(weight, at * rows, rows) for at in order], axis=0
        )

    wg, wu = (rolled(w, 2, (core, 1 - core)) for w in (wg, wu))
    w_out_rolled = rolled(w_out, groups, [(chip + groups - d) % groups for d in range(groups)])
    wd_theirs, wd_mine, wg, wu, w_out_rolled = lax.optimization_barrier(
        (by_core(1 - core), by_core(core), wg, wu, w_out_rolled)
    )
    (rows,), ((_, count),) = outgoing, CHUNKS
    shaped = rows.reshape(experts, count, rows.shape[1])
    got = lax.all_to_all(shaped, EP, split_axis=0, concat_axis=0, tiled=True)
    own = got.reshape(rows.shape)
    other = lax.ppermute(own, "c", swap)
    line = lax.all_to_all(message, EP, split_axis=0, concat_axis=0, tiled=True)
    x = lax.optimization_barrier(jnp.concatenate([own, other], axis=1))
    hidden = (jax.nn.silu(dot(x, wg)) * dot(x, wu)).astype(BF)
    for_partner = dot(hidden, wd_theirs).astype(BF)
    received = lax.ppermute(for_partner, "c", swap)
    mine = lax.optimization_barrier(dot(hidden, wd_mine).astype(BF))
    received, _ = lax.optimization_barrier((received, line))
    cols = received.shape[1] // groups
    pair = jnp.stack(
        [
            (mine[:, at : at + cols].astype(F32) + received[:, at : at + cols].astype(F32)).astype(BF)
            for at in range(0, received.shape[1], cols)
        ]
    )
    shaped = pair.reshape((groups * experts, count, cols))
    back = lax.all_to_all(shaped, ("y", "z", "x"), split_axis=0, concat_axis=0, tiled=True)
    back = back.reshape(pair.shape)
    summed = sum(back[g].astype(F32) for g in range(groups)).astype(BF)
    returned = [summed]
    keep, give = finish(idx, o, qf, qb, line, head_gain[None], groups, deps=(shaped,))
    given = lax.ppermute(give, "c", swap)
    lower = jnp.where(core == 0, keep, given)
    upper = jnp.where(core == 0, given, keep)
    parts = [jnp.stack([lower[d], upper[d]]) for d in range(groups)]
    moved = [parts[0]] + [lax.ppermute(parts[d], "y", ring(groups, d)) for d in range(1, groups)]
    moe_out = combine(routes, route_logits, returned, experts)
    features = jnp.concatenate([part[i] for part in moved for i in range(2)], axis=1)
    mixed_out = dot(features, w_out_rolled).astype(BF)
    return (mixed_out, moe_out)


def solution(mesh):
    finer = Mesh(mesh.devices.reshape(4, 4, 4, 2), ALL)

    return jax.shard_map(
        body,
        mesh=finer,
        in_specs=(
            P(EP, None),
            P(),
            P(None, TP),
            P(None, TP),
            P(None, TP),
            P(None, TP),
            P(TP),
            P(EP, TP),
            P(),
            P(),
            P(EP, None),
            P(),
            P(EP, None),
            P(EP, None),
            P(EP, None, TP),
            P(EP, None, TP),
            P(EP, TP, None),
        ),
        out_specs=(P(ALL, None), P(EP, TP)),
        check_vma=False,
    )
```

```python
import functools

import jax
import jax.numpy as jnp
from jax import lax
from jax.experimental import pallas as pl
from jax.experimental.pallas import tpu as pltpu
from jax.sharding import Mesh
from jax.sharding import PartitionSpec as P

DK = 128
DV = 128
BLK = 128
EP = ("z", "x")
TP = ("y", "c")
ALL = ("z", "x", "y", "c")
EPSILON = 1e-06
BF = jnp.bfloat16
F32 = jnp.float32
CHUNKS = ((0, 40), (40, 32))
COST_UNIT = 250e6


def params(mib, *semantics):
    return pltpu.CompilerParams(
        dimension_semantics=semantics if semantics else None, vmem_limit_bytes=mib * 1024 * 1024
    )


def cost(micros):
    return pl.CostEstimate(flops=int(micros * COST_UNIT), transcendentals=0, bytes_accessed=0)


def after(kernel, at, deps):
    def run(*refs):
        kernel(*refs[:at], *refs[at + len(deps) :])

    return run


def any_specs(deps):
    return [pl.BlockSpec(memory_space=pl.ANY) for _ in deps]


def dot(a, b):
    return jnp.dot(a, b, preferred_element_type=F32)


def dot_nt(a, b):
    return lax.dot_general(a, b, (((1,), (1,)), ((), ())), preferred_element_type=F32)


def dot_tn(a, b):
    return lax.dot_general(a, b, (((0,), (0,)), ((), ())), preferred_element_type=F32)


def rms_scale(floats):
    return lax.rsqrt(jnp.mean(floats * floats, axis=-1, keepdims=True) + EPSILON)


def dispatch_kernel(idx_ref, tok_ref, gain_ref, routes_ref, *outs, chunks, experts):
    half = tok_ref.shape[1] // 2
    rows = tok_ref.shape[0]
    scale = rms_scale(tok_ref[...].astype(F32))
    start = pl.multiple_of(idx_ref[0] * half, half)
    own = tok_ref[:, pl.ds(start, half)].astype(F32)
    normed = (own * scale * gain_ref[:, pl.ds(start, half)]).astype(BF)
    e0 = routes_ref[0:1, :]
    e1 = routes_ref[1:2, :]
    expert_iota = lax.broadcasted_iota(jnp.int32, (experts, rows), 0)
    oh0 = (expert_iota == e0).astype(F32)
    oh1 = (expert_iota == e1).astype(F32)
    earlier = (
        lax.broadcasted_iota(jnp.int32, (rows, rows), 0)
        < lax.broadcasted_iota(jnp.int32, (rows, rows), 1)
    ).astype(F32)
    before = dot((oh0 + oh1).astype(BF), earlier.astype(BF))
    slot0 = jnp.sum(oh0 * before, axis=0, keepdims=True).astype(jnp.int32)
    slot1 = jnp.sum(oh1 * (before + oh0), axis=0, keepdims=True).astype(jnp.int32)
    for out, (first, count) in zip(outs, chunks):
        total = experts * count

        def place(expert, slot):
            inside = (slot >= first) & (slot < first + count)
            return jnp.where(inside, expert * count + slot - first, -1)

        p0 = place(e0, slot0)
        p1 = place(e1, slot1)
        row_iota = lax.broadcasted_iota(jnp.int32, (total, rows), 0)
        chosen = ((row_iota == p0) | (row_iota == p1)).astype(F32).astype(BF)
        out[...] = dot(chosen, normed).astype(BF)


def dispatch(idx, tokens, gain, routes_t, experts):
    half = tokens.shape[1] // 2
    return pl.pallas_call(
        functools.partial(dispatch_kernel, chunks=CHUNKS, experts=experts),
        out_shape=tuple(jax.ShapeDtypeStruct((experts * n, half), BF) for _, n in CHUNKS),
        in_specs=[
            pl.BlockSpec(memory_space=pltpu.SMEM),
            pl.BlockSpec(memory_space=pltpu.VMEM),
            pl.BlockSpec(memory_space=pltpu.VMEM),
            pl.BlockSpec(memory_space=pltpu.VMEM),
        ],
        out_specs=tuple(pl.BlockSpec(memory_space=pltpu.VMEM) for _ in CHUNKS),
        compiler_params=params(56),
        cost_estimate=cost(5),
        name="dispatch",
    )(idx, tokens, gain, routes_t)


def tri_sum(tri, g):
    high = g.astype(BF)
    low = (g - high.astype(F32)).astype(BF)
    return dot(tri, high) + dot(tri, low)


def local_kernel(
    idx_ref,
    x_ref,
    gain_ref,
    wq_ref,
    wf_ref,
    wb_ref,
    wv_ref,
    floor_ref,
    shift_ref,
    wg_ref,
    wu_ref,
    wd_ref,
    wo_ref,
    o_ref,
    qf_ref,
    qb_ref,
    msg_ref,
    wg_out,
    wu_out,
    theirs_out,
    mine_out,
    wo_out,
    q_s,
    v_s,
    kb_s,
    gb_s,
    st_s,
    off_s,
    kept_s,
    wg_s,
    wu_s,
    theirs_s,
    mine_s,
    wo_s,
    sems,
    *,
    steps,
    rows,
    heads,
    groups,
):
    step = pl.program_id(0)
    width = heads * DK
    core, chip = idx_ref[0], idx_ref[1]
    loads = []

    def load(source, target):
        loads.append(pltpu.make_async_copy(source, target, sems.at[len(loads)]))

    half = wg_ref.shape[0] // 2
    for i in range(2):
        taken = pl.ds(pl.multiple_of(lax.rem(core + i, 2) * half, half), half)
        put = slice(i * half, (i + 1) * half)
        load(wg_ref.at[taken, :], wg_s.at[put, :])
        load(wu_ref.at[taken, :], wu_s.at[put, :])
    cols = wd_ref.shape[1] // (2 * groups)
    share = wo_ref.shape[0] // groups
    for d in range(groups):
        put = slice(d * cols, (d + 1) * cols)
        block = 2 * lax.rem(chip + d, groups)
        for target, which in ((theirs_s, 1 - core), (mine_s, core)):
            taken = pl.ds(pl.multiple_of((block + which) * cols, cols), cols)
            load(wd_ref.at[:, taken], target.at[:, put])
        source = lax.rem(chip + groups - d, groups)
        taken = pl.ds(pl.multiple_of(source * share, share), share)
        load(wo_ref.at[taken, :], wo_s.at[d * share : (d + 1) * share, :])
    stores = [
        pltpu.make_async_copy(source, target, sems.at[len(loads) + i])
        for i, (source, target) in enumerate(
            (
                (wg_s, wg_out),
                (wu_s, wu_out),
                (theirs_s, theirs_out),
                (mine_s, mine_out),
                (wo_s, wo_out),
            )
        )
    ]

    @pl.when(step == 0)
    def _():
        for copy in loads:
            copy.start()

    @pl.when(step == steps // 2)
    def _():
        for copy in loads:
            copy.wait()
        for copy in stores:
            copy.start()

    @pl.when(step == 0)
    def _():
        st_s[...] = jnp.zeros_like(st_s)
        off_s[...] = jnp.zeros_like(off_s)
        kept_s[...] = jnp.zeros_like(kept_s)

    x = x_ref[...].astype(F32)
    normed = (x * rms_scale(x) * gain_ref[...]).astype(BF)

    def project(w_ref):
        return dot(normed, w_ref[...]).astype(BF)

    q_pre = project(wq_ref).astype(F32)
    queries = q_pre * jax.nn.sigmoid(q_pre)
    values = project(wv_ref)
    shift = shift_ref[...]
    shift_wide = jnp.concatenate(
        [jnp.broadcast_to(shift[:, h : h + 1], (rows, DK)) for h in range(heads)], axis=1
    )
    room = 1.0 - floor_ref[...]

    def decay(w_ref):
        keys = room * (1.0 - jax.nn.sigmoid(project(w_ref).astype(F32)))
        return keys, jnp.log1p(-keys) + shift_wide

    keys_f, logs_f = decay(wf_ref)
    keys_b, logs_b = decay(wb_ref)
    base = pl.multiple_of(step * rows, rows)
    q_s[pl.ds(base, rows), :] = queries
    v_s[pl.ds(base, rows), :] = values
    kb_s[pl.ds(base, rows), :] = keys_b
    gb_s[pl.ds(base, rows), :] = logs_b

    row_iota = lax.broadcasted_iota(jnp.int32, (BLK, BLK), 0)
    col_iota = lax.broadcasted_iota(jnp.int32, (BLK, BLK), 1)
    lower = row_iota >= col_iota
    upper = row_iota <= col_iota
    lower_one = lower.astype(F32).astype(BF)
    upper_one = upper.astype(F32).astype(BF)

    def block(q, k, v, g, tri_one, mask, end_row, states, offset):
        run = tri_sum(tri_one, g)
        end = run[end_row : end_row + 1, :]
        grown = q * jnp.exp(run)
        grown_b = grown.astype(BF)
        shrunk = (k * jnp.exp(-run)).astype(BF)
        closing = (k * jnp.exp(end - run)).astype(BF)
        kept = jnp.exp(end)
        result = []
        new_states = []
        for h in range(heads):
            lanes = slice(h * DK, (h + 1) * DK)
            scores = jnp.where(mask, dot_nt(grown_b[:, lanes], shrunk[:, lanes]), 0.0).astype(BF)
            st = states[h]
            result.append(
                dot(scores, v[:, lanes]) + dot_nt(grown_b[:, lanes], st.astype(BF))
            )
            new_states.append(st * kept[:, lanes] + dot_tn(v[:, lanes], closing[:, lanes]))
        carried = (grown * jnp.exp(offset)).astype(BF)
        return jnp.concatenate(result, axis=1), new_states, carried, offset + end

    def write_message(way, states, total):
        kept = jnp.exp(total)
        high = kept.astype(BF).astype(F32)
        for h in range(heads):
            lanes = slice(h * DK, (h + 1) * DK)
            kept_s[h : h + 1, :] = high[:, lanes]
            kept_s[heads + h : heads + h + 1, :] = (kept - high)[:, lanes]
        whole = jnp.concatenate(list(states) + [kept_s[...]], axis=0).astype(BF)

        def write(target, _):
            msg_ref[target] = whole
            return 0

        here = idx_ref[2]
        if way == 0:
            lax.fori_loop(here, msg_ref.shape[0], write, 0)
        else:
            lax.fori_loop(0, here, write, 0)

    states = [st_s[h] for h in range(heads)]
    offset = off_s[...]
    for b in range(rows // BLK):
        rs = slice(b * BLK, (b + 1) * BLK)
        result, states, carried, offset = block(
            queries[rs], keys_f[rs], values[rs], logs_f[rs], lower_one, lower, BLK - 1, states, offset
        )
        at = pl.multiple_of(base + b * BLK, BLK)
        o_ref[pl.ds(at, BLK), :] = result
        qf_ref[pl.ds(at, BLK), :] = carried
    for h in range(heads):
        st_s[h] = states[h]
    off_s[...] = offset

    @pl.when(step == steps - 1)
    def _():
        write_message(0, states, offset)
        back = [jnp.zeros((DV, DK), F32) for _ in range(heads)]
        total = jnp.zeros((1, width), F32)
        for b in reversed(range(steps * rows // BLK)):
            rs = slice(b * BLK, (b + 1) * BLK)
            result, back, carried, total = block(
                q_s[rs, :], kb_s[rs, :], v_s[rs, :], gb_s[rs, :], upper_one, upper, 0, back, total
            )
            o_ref[rs, :] = o_ref[rs, :] + result
            qb_ref[rs, :] = carried
        write_message(1, back, total)
        for copy in stores:
            copy.wait()


def local_sweeps(
    idx, tokens, gain, wq, wf, wb, wv, floor, shift, wg, wu, wd, wo, segments, groups, deps=()
):
    seg, model = tokens.shape
    width = wq.shape[1]
    heads = width // DK
    rows = 256
    steps = seg // rows
    whole = lambda shape: pl.BlockSpec(shape, lambda i: tuple(0 for _ in shape))
    return pl.pallas_call(
        after(
            functools.partial(local_kernel, steps=steps, rows=rows, heads=heads, groups=groups),
            13,
            deps,
        ),
        grid=(steps,),
        out_shape=(
            jax.ShapeDtypeStruct((seg, width), F32),
            jax.ShapeDtypeStruct((seg, width), BF),
            jax.ShapeDtypeStruct((seg, width), BF),
            jax.ShapeDtypeStruct((segments, heads * DV + 8, DK), BF),
            jax.ShapeDtypeStruct(wg.shape, BF),
            jax.ShapeDtypeStruct(wu.shape, BF),
            jax.ShapeDtypeStruct((wd.shape[0], wd.shape[1] // 2), BF),
            jax.ShapeDtypeStruct((wd.shape[0], wd.shape[1] // 2), BF),
            jax.ShapeDtypeStruct(wo.shape, BF),
        ),
        in_specs=[
            pl.BlockSpec(memory_space=pltpu.SMEM),
            pl.BlockSpec((rows, model), lambda i: (i, 0)),
            whole((1, model)),
            whole((model, width)),
            whole((model, width)),
            whole((model, width)),
            whole((model, width)),
            whole((1, width)),
            pl.BlockSpec((rows, heads), lambda i: (i, 0)),
            *any_specs((wg, wu, wd, wo)),
            *any_specs(deps),
        ],
        out_specs=(
            whole((seg, width)),
            whole((seg, width)),
            whole((seg, width)),
            whole((segments, heads * DV + 8, DK)),
            *any_specs(range(5)),
        ),
        scratch_shapes=[
            pltpu.VMEM((seg, width), F32),
            pltpu.VMEM((seg, width), BF),
            pltpu.VMEM((seg, width), F32),
            pltpu.VMEM((seg, width), F32),
            pltpu.VMEM((heads, DV, DK), F32),
            pltpu.VMEM((1, width), F32),
            pltpu.VMEM((8, DK), F32),
            pltpu.VMEM(wg.shape, BF),
            pltpu.VMEM(wu.shape, BF),
            pltpu.VMEM((wd.shape[0], wd.shape[1] // 2), BF),
            pltpu.VMEM((wd.shape[0], wd.shape[1] // 2), BF),
            pltpu.VMEM(wo.shape, BF),
            pltpu.SemaphoreType.DMA((9 + 3 * groups,)),
        ],
        compiler_params=params(48, "arbitrary"),
        cost_estimate=cost(17),
        name="local_sweeps",
    )(idx, tokens, gain, wq, wf, wb, wv, floor, shift, wg, wu, wd, wo, *deps)


def finish_kernel(idx_ref, *refs, heads):
    line_ref, gain_ref, *outs, states_ref = refs[6:]
    here = idx_ref[2]
    count = line_ref.shape[0]

    @pl.when(pl.program_id(0) == 0)
    def _():
        zeros = tuple(jnp.zeros((DV, DK), F32) for _ in range(heads))

        def join(source, states):
            new = []
            for h, state in enumerate(states):
                tail = line_ref[source, heads * DV :, :].astype(F32)
                kept = tail[h : h + 1, :] + tail[heads + h : heads + h + 1, :]
                new.append(
                    state * kept + line_ref[source, h * DV : (h + 1) * DV, :].astype(F32)
                )
            return tuple(new)

        ahead = lax.fori_loop(0, here, join, zeros)
        behind = lax.fori_loop(0, count - 1 - here, lambda i, st: join(count - 1 - i, st), zeros)
        for p, state in enumerate(ahead + behind):
            states_ref[p * DV : (p + 1) * DV, :] = state.astype(BF)

    for (o_ref, qf_ref, qb_ref), out_ref in zip((refs[0:3], refs[3:6]), outs):
        for h in range(heads):
            lanes = slice(h * DK, (h + 1) * DK)
            ahead = states_ref[h * DV : (h + 1) * DV, :]
            behind = states_ref[(heads + h) * DV : (heads + h + 1) * DV, :]
            o = (
                o_ref[:, lanes]
                + dot_nt(qf_ref[:, lanes], ahead)
                + dot_nt(qb_ref[:, lanes], behind)
            )
            out_ref[0, :, lanes] = (o * rms_scale(o) * gain_ref[...]).astype(BF)


def finish(idx, o, qf, qb, line, gain, groups, deps=()):
    seg, width = o.shape
    rows = seg // (2 * groups)

    def tile(other):
        return pl.BlockSpec(
            (rows, width), lambda d, s: (2 * ((s[1] + d) % groups) + jnp.bitwise_xor(s[0], other), 0)
        )

    out = pl.BlockSpec((1, rows, width), lambda d, s: (d, 0, 0))
    shape = jax.ShapeDtypeStruct((groups, rows, width), BF)
    return pl.pallas_call(
        after(functools.partial(finish_kernel, heads=width // DK), 9, deps),
        grid_spec=pltpu.PrefetchScalarGridSpec(
            num_scalar_prefetch=1,
            grid=(groups,),
            in_specs=[
                *(tile(other) for other in (0, 0, 0, 1, 1, 1)),
                pl.BlockSpec(line.shape, lambda d, s: (0, 0, 0)),
                pl.BlockSpec(gain.shape, lambda d, s: (0, 0)),
                *any_specs(deps),
            ],
            out_specs=(out, out),
            scratch_shapes=[pltpu.VMEM((2 * width, DK), BF)],
        ),
        out_shape=(shape, shape),
        compiler_params=params(12, "arbitrary"),
        cost_estimate=cost(4),
        name="finish",
    )(idx, o, qf, qb, o, qf, qb, line, gain, *deps)


def combine_kernel(routes_ref, logits_ref, *refs, chunks, experts):
    returned, out_ref = refs[:-1], refs[-1]
    rows = routes_ref.shape[0]
    expert_iota = lax.broadcasted_iota(jnp.int32, (rows, experts), 1)
    e0 = routes_ref[:, 0:1]
    e1 = routes_ref[:, 1:2]
    oh0 = (expert_iota == e0).astype(F32)
    oh1 = (expert_iota == e1).astype(F32)
    earlier = (
        lax.broadcasted_iota(jnp.int32, (rows, rows), 1)
        < lax.broadcasted_iota(jnp.int32, (rows, rows), 0)
    ).astype(F32)
    before = dot(earlier.astype(BF), (oh0 + oh1).astype(BF))
    slot0 = jnp.sum(oh0 * before, axis=1, keepdims=True).astype(jnp.int32)
    slot1 = jnp.sum(oh1 * (before + oh0), axis=1, keepdims=True).astype(jnp.int32)
    logits = logits_ref[...]
    gap = logits[:, 0:1] - logits[:, 1:2]

    def picked(expert, slot):
        total = 0.0
        for result, (first, count) in zip(returned, chunks):
            inside = (slot >= first) & (slot < first + count)
            place = jnp.where(inside, expert * count + slot - first, -1)
            lane_iota = lax.broadcasted_iota(jnp.int32, (rows, experts * count), 1)
            chosen = (lane_iota == place).astype(F32).astype(BF)
            total = total + dot(chosen, result[...])
        return total

    out_ref[...] = (
        picked(e0, slot0) * jax.nn.sigmoid(gap) + picked(e1, slot1) * jax.nn.sigmoid(-gap)
    ).astype(BF)


def combine(routes, logits, returned, experts):
    rows = routes.shape[0]
    cols = returned[0].shape[1]
    return pl.pallas_call(
        functools.partial(combine_kernel, chunks=((0, sum(n for _, n in CHUNKS)),), experts=experts),
        out_shape=jax.ShapeDtypeStruct((rows, cols), BF),
        in_specs=[pl.BlockSpec(memory_space=pltpu.VMEM) for _ in range(2 + len(returned))],
        out_specs=pl.BlockSpec(memory_space=pltpu.VMEM),
        compiler_params=params(12),
        cost_estimate=cost(4),
        name="combine",
    )(routes, logits, *returned)


def ring(count, shift):
    return [(i, (i + shift) % count) for i in range(count)]


def body(
    mix_tokens,
    mix_gain,
    w_query,
    w_forget_fwd,
    w_forget_bwd,
    w_value,
    decay_floor,
    decay_shift,
    head_gain,
    w_out,
    moe_tokens,
    moe_gain,
    routes,
    route_logits,
    w_expert_gate,
    w_expert_up,
    w_expert_down,
):
    experts = lax.axis_size(EP)
    groups = lax.axis_size("y")
    core, chip = lax.axis_index("c"), lax.axis_index("y")
    idx = jnp.stack([core, chip, lax.axis_index(EP)]).astype(jnp.int32)
    swap = [(0, 1), (1, 0)]
    wg, wu, wd = w_expert_gate[0], w_expert_up[0], w_expert_down[0]

    outgoing = dispatch(idx, moe_tokens, moe_gain[None], routes.T, experts)
    o, qf, qb, message, wg, wu, wd_theirs, wd_mine, w_out_rolled = local_sweeps(
        idx,
        mix_tokens,
        mix_gain[None],
        w_query,
        w_forget_fwd,
        w_forget_bwd,
        w_value,
        decay_floor[None],
        decay_shift,
        wg,
        wu,
        wd,
        w_out,
        experts,
        groups,
        deps=outgoing,
    )
    landed = []
    arrived = []
    for rows, (_, count) in zip(outgoing, CHUNKS):
        shaped = rows.reshape(experts, count, rows.shape[1])
        got = lax.all_to_all(shaped, EP, split_axis=0, concat_axis=0, tiled=True)
        arrived.append(got.reshape(rows.shape))
    arrived[-1], message = lax.optimization_barrier((arrived[-1], message))
    line = lax.all_to_all(message, EP, split_axis=0, concat_axis=0, tiled=True)
    for own in arrived:
        other = lax.ppermute(own, "c", swap)
        x = lax.optimization_barrier(jnp.concatenate([own, other], axis=1))
        hidden = (jax.nn.silu(dot(x, wg)) * dot(x, wu)).astype(BF)
        for_partner = dot(hidden, wd_theirs).astype(BF)
        received = lax.ppermute(for_partner, "c", swap)
        mine = lax.optimization_barrier(dot(hidden, wd_mine).astype(BF))
        cols = received.shape[1] // groups
        pair = [
            (
                mine[:, at : at + cols].astype(F32) + received[:, at : at + cols].astype(F32)
            ).astype(BF)
            for at in range(0, received.shape[1], cols)
        ]
        landed.append([pair[0]] + [lax.ppermute(pair[d], "y", ring(groups, d)) for d in (2, 1, 3)])
    keep, give = finish(idx, o, qf, qb, line, head_gain[None], groups, deps=tuple(pair[1:]))
    given = lax.ppermute(give, "c", swap)
    lower = jnp.where(core == 0, keep, given)
    upper = jnp.where(core == 0, given, keep)
    parts = [jnp.stack([lower[d], upper[d]]) for d in range(groups)]
    moved = [parts[0]] + [lax.ppermute(parts[d], "y", ring(groups, d)) for d in range(1, groups)]
    shaped = jnp.concatenate(
        [
            sum(part.astype(F32) for part in chunk).astype(BF).reshape(experts, -1, cols)
            for chunk in landed
        ],
        axis=1,
    )
    back = lax.all_to_all(shaped, EP, split_axis=0, concat_axis=0, tiled=True)
    returned = [back.reshape(-1, cols)]
    features = jnp.concatenate([part[i] for part in moved for i in range(2)], axis=1)
    mixed_out = dot(features, w_out_rolled).astype(BF)
    moe_out = combine(routes, route_logits, returned, experts)
    return (mixed_out, moe_out)


def solution(mesh):
    finer = Mesh(mesh.devices.reshape(4, 4, 4, 2), ALL)

    return jax.shard_map(
        body,
        mesh=finer,
        in_specs=(
            P(EP, None),
            P(),
            P(None, TP),
            P(None, TP),
            P(None, TP),
            P(None, TP),
            P(TP),
            P(EP, TP),
            P(),
            P(),
            P(EP, None),
            P(),
            P(EP, None),
            P(EP, None),
            P(EP, None, TP),
            P(EP, None, TP),
            P(EP, TP, None),
        ),
        out_specs=(P(ALL, None), P(EP, TP)),
        check_vma=False,
    )
```

```python
import functools

import jax
import jax.numpy as jnp
from jax import lax
from jax.experimental import pallas as pl
from jax.experimental.pallas import tpu as pltpu
from jax.sharding import Mesh
from jax.sharding import PartitionSpec as P

DK = 128
DV = 128
BLK = 128
EP = ("z", "x")
TP = ("y", "c")
ALL = ("z", "x", "y", "c")
EPSILON = 1e-06
BF = jnp.bfloat16
F32 = jnp.float32
CHUNKS = ((0, 40), (40, 32))
COST_UNIT = 250e6


def params(mib, *semantics):
    return pltpu.CompilerParams(
        dimension_semantics=semantics if semantics else None, vmem_limit_bytes=mib * 1024 * 1024
    )


def cost(micros):
    return pl.CostEstimate(flops=int(micros * COST_UNIT), transcendentals=0, bytes_accessed=0)


def after(kernel, at, deps):
    def run(*refs):
        kernel(*refs[:at], *refs[at + len(deps) :])

    return run


def any_specs(deps):
    return [pl.BlockSpec(memory_space=pl.ANY) for _ in deps]


def dot(a, b):
    return jnp.dot(a, b, preferred_element_type=F32)


def dot_nt(a, b):
    return lax.dot_general(a, b, (((1,), (1,)), ((), ())), preferred_element_type=F32)


def dot_tn(a, b):
    return lax.dot_general(a, b, (((0,), (0,)), ((), ())), preferred_element_type=F32)


def rms_scale(floats):
    return lax.rsqrt(jnp.mean(floats * floats, axis=-1, keepdims=True) + EPSILON)


def dispatch_kernel(idx_ref, tok_ref, gain_ref, routes_ref, *outs, chunks, experts):
    half = tok_ref.shape[1] // 2
    rows = tok_ref.shape[0]
    scale = rms_scale(tok_ref[...].astype(F32))
    start = pl.multiple_of(idx_ref[0] * half, half)
    own = tok_ref[:, pl.ds(start, half)].astype(F32)
    normed = (own * scale * gain_ref[:, pl.ds(start, half)]).astype(BF)
    e0 = routes_ref[0:1, :]
    e1 = routes_ref[1:2, :]
    expert_iota = lax.broadcasted_iota(jnp.int32, (experts, rows), 0)
    oh0 = (expert_iota == e0).astype(F32)
    oh1 = (expert_iota == e1).astype(F32)
    earlier = (
        lax.broadcasted_iota(jnp.int32, (rows, rows), 0)
        < lax.broadcasted_iota(jnp.int32, (rows, rows), 1)
    ).astype(F32)
    before = dot((oh0 + oh1).astype(BF), earlier.astype(BF))
    slot0 = jnp.sum(oh0 * before, axis=0, keepdims=True).astype(jnp.int32)
    slot1 = jnp.sum(oh1 * (before + oh0), axis=0, keepdims=True).astype(jnp.int32)
    for out, (first, count) in zip(outs, chunks):
        total = experts * count

        def place(expert, slot):
            inside = (slot >= first) & (slot < first + count)
            return jnp.where(inside, expert * count + slot - first, -1)

        p0 = place(e0, slot0)
        p1 = place(e1, slot1)
        row_iota = lax.broadcasted_iota(jnp.int32, (total, rows), 0)
        chosen = ((row_iota == p0) | (row_iota == p1)).astype(F32).astype(BF)
        out[...] = dot(chosen, normed).astype(BF)


def dispatch(idx, tokens, gain, routes_t, experts):
    half = tokens.shape[1] // 2
    return pl.pallas_call(
        functools.partial(dispatch_kernel, chunks=CHUNKS, experts=experts),
        out_shape=tuple(jax.ShapeDtypeStruct((experts * n, half), BF) for _, n in CHUNKS),
        in_specs=[
            pl.BlockSpec(memory_space=pltpu.SMEM),
            pl.BlockSpec(memory_space=pltpu.VMEM),
            pl.BlockSpec(memory_space=pltpu.VMEM),
            pl.BlockSpec(memory_space=pltpu.VMEM),
        ],
        out_specs=tuple(pl.BlockSpec(memory_space=pltpu.VMEM) for _ in CHUNKS),
        compiler_params=params(56),
        cost_estimate=cost(5),
        name="dispatch",
    )(idx, tokens, gain, routes_t)


def tri_sum(tri, g):
    high = g.astype(BF)
    low = (g - high.astype(F32)).astype(BF)
    return dot(tri, high) + dot(tri, low)


def local_kernel(
    idx_ref,
    x_ref,
    gain_ref,
    wq_ref,
    wf_ref,
    wb_ref,
    wv_ref,
    floor_ref,
    shift_ref,
    wg_ref,
    wu_ref,
    wd_ref,
    o_ref,
    qf_ref,
    qb_ref,
    msg_ref,
    wg_out,
    wu_out,
    theirs_out,
    mine_out,
    q_s,
    v_s,
    kb_s,
    gb_s,
    st_s,
    off_s,
    kept_s,
    wg_s,
    wu_s,
    theirs_s,
    mine_s,
    sems,
    *,
    steps,
    rows,
    heads,
    groups,
):
    step = pl.program_id(0)
    width = heads * DK
    core, chip = idx_ref[0], idx_ref[1]
    loads = []

    def load(source, target):
        loads.append(pltpu.make_async_copy(source, target, sems.at[len(loads)]))

    half = wg_ref.shape[0] // 2
    for i in range(2):
        taken = pl.ds(pl.multiple_of(lax.rem(core + i, 2) * half, half), half)
        put = slice(i * half, (i + 1) * half)
        load(wg_ref.at[taken, :], wg_s.at[put, :])
        load(wu_ref.at[taken, :], wu_s.at[put, :])
    cols = wd_ref.shape[1] // (2 * groups)
    for d in range(groups):
        put = slice(d * cols, (d + 1) * cols)
        block = 2 * lax.rem(chip + d, groups)
        for target, which in ((theirs_s, 1 - core), (mine_s, core)):
            taken = pl.ds(pl.multiple_of((block + which) * cols, cols), cols)
            load(wd_ref.at[:, taken], target.at[:, put])
    stores = [
        pltpu.make_async_copy(source, target, sems.at[len(loads) + i])
        for i, (source, target) in enumerate(
            (
                (wg_s, wg_out),
                (wu_s, wu_out),
                (theirs_s, theirs_out),
                (mine_s, mine_out),
            )
        )
    ]

    @pl.when(step == 0)
    def _():
        for copy in loads:
            copy.start()

    @pl.when(step == steps // 2)
    def _():
        for copy in loads:
            copy.wait()
        for copy in stores:
            copy.start()

    @pl.when(step == 0)
    def _():
        st_s[...] = jnp.zeros_like(st_s)
        off_s[...] = jnp.zeros_like(off_s)
        kept_s[...] = jnp.zeros_like(kept_s)

    x = x_ref[...].astype(F32)
    normed = (x * rms_scale(x) * gain_ref[...]).astype(BF)

    def project(w_ref):
        return dot(normed, w_ref[...]).astype(BF)

    q_pre = project(wq_ref).astype(F32)
    queries = q_pre * jax.nn.sigmoid(q_pre)
    values = project(wv_ref)
    shift = shift_ref[...]
    shift_wide = jnp.concatenate(
        [jnp.broadcast_to(shift[:, h : h + 1], (rows, DK)) for h in range(heads)], axis=1
    )
    room = 1.0 - floor_ref[...]

    def decay(w_ref):
        keys = room * (1.0 - jax.nn.sigmoid(project(w_ref).astype(F32)))
        return keys, jnp.log1p(-keys) + shift_wide

    keys_f, logs_f = decay(wf_ref)
    keys_b, logs_b = decay(wb_ref)
    base = pl.multiple_of(step * rows, rows)
    q_s[pl.ds(base, rows), :] = queries
    v_s[pl.ds(base, rows), :] = values
    kb_s[pl.ds(base, rows), :] = keys_b
    gb_s[pl.ds(base, rows), :] = logs_b

    row_iota = lax.broadcasted_iota(jnp.int32, (BLK, BLK), 0)
    col_iota = lax.broadcasted_iota(jnp.int32, (BLK, BLK), 1)
    lower = row_iota >= col_iota
    upper = row_iota <= col_iota
    lower_one = lower.astype(F32).astype(BF)
    upper_one = upper.astype(F32).astype(BF)

    def block(q, k, v, g, tri_one, mask, end_row, states, offset):
        run = tri_sum(tri_one, g)
        end = run[end_row : end_row + 1, :]
        grown = q * jnp.exp(run)
        grown_b = grown.astype(BF)
        shrunk = (k * jnp.exp(-run)).astype(BF)
        closing = (k * jnp.exp(end - run)).astype(BF)
        kept = jnp.exp(end)
        result = []
        new_states = []
        for h in range(heads):
            lanes = slice(h * DK, (h + 1) * DK)
            scores = jnp.where(mask, dot_nt(grown_b[:, lanes], shrunk[:, lanes]), 0.0).astype(BF)
            st = states[h]
            result.append(
                dot(scores, v[:, lanes]) + dot_nt(grown_b[:, lanes], st.astype(BF))
            )
            new_states.append(st * kept[:, lanes] + dot_tn(v[:, lanes], closing[:, lanes]))
        carried = (grown * jnp.exp(offset)).astype(BF)
        return jnp.concatenate(result, axis=1), new_states, carried, offset + end

    def write_message(way, states, total):
        kept = jnp.exp(total)
        high = kept.astype(BF).astype(F32)
        for h in range(heads):
            lanes = slice(h * DK, (h + 1) * DK)
            kept_s[h : h + 1, :] = high[:, lanes]
            kept_s[heads + h : heads + h + 1, :] = (kept - high)[:, lanes]
        whole = jnp.concatenate(list(states) + [kept_s[...]], axis=0).astype(BF)

        def write(target, _):
            msg_ref[target] = whole
            return 0

        here = idx_ref[2]
        if way == 0:
            lax.fori_loop(here, msg_ref.shape[0], write, 0)
        else:
            lax.fori_loop(0, here, write, 0)

    states = [st_s[h] for h in range(heads)]
    offset = off_s[...]
    for b in range(rows // BLK):
        rs = slice(b * BLK, (b + 1) * BLK)
        result, states, carried, offset = block(
            queries[rs], keys_f[rs], values[rs], logs_f[rs], lower_one, lower, BLK - 1, states, offset
        )
        at = pl.multiple_of(base + b * BLK, BLK)
        o_ref[pl.ds(at, BLK), :] = result
        qf_ref[pl.ds(at, BLK), :] = carried
    for h in range(heads):
        st_s[h] = states[h]
    off_s[...] = offset

    @pl.when(step == steps - 1)
    def _():
        write_message(0, states, offset)
        back = [jnp.zeros((DV, DK), F32) for _ in range(heads)]
        total = jnp.zeros((1, width), F32)
        for b in reversed(range(steps * rows // BLK)):
            rs = slice(b * BLK, (b + 1) * BLK)
            result, back, carried, total = block(
                q_s[rs, :], kb_s[rs, :], v_s[rs, :], gb_s[rs, :], upper_one, upper, 0, back, total
            )
            o_ref[rs, :] = o_ref[rs, :] + result
            qb_ref[rs, :] = carried
        write_message(1, back, total)
        for copy in stores:
            copy.wait()


def local_sweeps(
    idx, tokens, gain, wq, wf, wb, wv, floor, shift, wg, wu, wd, segments, groups, deps=()
):
    seg, model = tokens.shape
    width = wq.shape[1]
    heads = width // DK
    rows = 256
    steps = seg // rows
    whole = lambda shape: pl.BlockSpec(shape, lambda i: tuple(0 for _ in shape))
    return pl.pallas_call(
        after(
            functools.partial(local_kernel, steps=steps, rows=rows, heads=heads, groups=groups),
            12,
            deps,
        ),
        grid=(steps,),
        out_shape=(
            jax.ShapeDtypeStruct((seg, width), F32),
            jax.ShapeDtypeStruct((seg, width), BF),
            jax.ShapeDtypeStruct((seg, width), BF),
            jax.ShapeDtypeStruct((segments, heads * DV + 8, DK), BF),
            jax.ShapeDtypeStruct(wg.shape, BF),
            jax.ShapeDtypeStruct(wu.shape, BF),
            jax.ShapeDtypeStruct((wd.shape[0], wd.shape[1] // 2), BF),
            jax.ShapeDtypeStruct((wd.shape[0], wd.shape[1] // 2), BF),
        ),
        in_specs=[
            pl.BlockSpec(memory_space=pltpu.SMEM),
            pl.BlockSpec((rows, model), lambda i: (i, 0)),
            whole((1, model)),
            whole((model, width)),
            whole((model, width)),
            whole((model, width)),
            whole((model, width)),
            whole((1, width)),
            pl.BlockSpec((rows, heads), lambda i: (i, 0)),
            *any_specs((wg, wu, wd)),
            *any_specs(deps),
        ],
        out_specs=(
            whole((seg, width)),
            whole((seg, width)),
            whole((seg, width)),
            whole((segments, heads * DV + 8, DK)),
            *any_specs(range(4)),
        ),
        scratch_shapes=[
            pltpu.VMEM((seg, width), F32),
            pltpu.VMEM((seg, width), BF),
            pltpu.VMEM((seg, width), F32),
            pltpu.VMEM((seg, width), F32),
            pltpu.VMEM((heads, DV, DK), F32),
            pltpu.VMEM((1, width), F32),
            pltpu.VMEM((8, DK), F32),
            pltpu.VMEM(wg.shape, BF),
            pltpu.VMEM(wu.shape, BF),
            pltpu.VMEM((wd.shape[0], wd.shape[1] // 2), BF),
            pltpu.VMEM((wd.shape[0], wd.shape[1] // 2), BF),
            pltpu.SemaphoreType.DMA((8 + 2 * groups,)),
        ],
        compiler_params=params(48, "arbitrary"),
        cost_estimate=cost(17),
        name="local_sweeps",
    )(idx, tokens, gain, wq, wf, wb, wv, floor, shift, wg, wu, wd, *deps)


def finish_kernel(idx_ref, *refs, heads):
    line_ref, gain_ref, *outs, states_ref = refs[6:]
    here = idx_ref[2]
    count = line_ref.shape[0]

    @pl.when(pl.program_id(0) == 0)
    def _():
        zeros = tuple(jnp.zeros((DV, DK), F32) for _ in range(heads))

        def join(source, states):
            new = []
            for h, state in enumerate(states):
                tail = line_ref[source, heads * DV :, :].astype(F32)
                kept = tail[h : h + 1, :] + tail[heads + h : heads + h + 1, :]
                new.append(
                    state * kept + line_ref[source, h * DV : (h + 1) * DV, :].astype(F32)
                )
            return tuple(new)

        ahead = lax.fori_loop(0, here, join, zeros)
        behind = lax.fori_loop(0, count - 1 - here, lambda i, st: join(count - 1 - i, st), zeros)
        for p, state in enumerate(ahead + behind):
            states_ref[p * DV : (p + 1) * DV, :] = state.astype(BF)

    for (o_ref, qf_ref, qb_ref), out_ref in zip((refs[0:3], refs[3:6]), outs):
        for h in range(heads):
            lanes = slice(h * DK, (h + 1) * DK)
            ahead = states_ref[h * DV : (h + 1) * DV, :]
            behind = states_ref[(heads + h) * DV : (heads + h + 1) * DV, :]
            o = (
                o_ref[:, lanes]
                + dot_nt(qf_ref[:, lanes], ahead)
                + dot_nt(qb_ref[:, lanes], behind)
            )
            out_ref[0, :, lanes] = (o * rms_scale(o) * gain_ref[...]).astype(BF)


def finish(idx, o, qf, qb, line, gain, groups, deps=()):
    seg, width = o.shape
    rows = seg // (2 * groups)

    def tile(other):
        return pl.BlockSpec(
            (rows, width), lambda d, s: (2 * ((s[1] + d) % groups) + jnp.bitwise_xor(s[0], other), 0)
        )

    out = pl.BlockSpec((1, rows, width), lambda d, s: (d, 0, 0))
    shape = jax.ShapeDtypeStruct((groups, rows, width), BF)
    return pl.pallas_call(
        after(functools.partial(finish_kernel, heads=width // DK), 9, deps),
        grid_spec=pltpu.PrefetchScalarGridSpec(
            num_scalar_prefetch=1,
            grid=(groups,),
            in_specs=[
                *(tile(other) for other in (0, 0, 0, 1, 1, 1)),
                pl.BlockSpec(line.shape, lambda d, s: (0, 0, 0)),
                pl.BlockSpec(gain.shape, lambda d, s: (0, 0)),
                *any_specs(deps),
            ],
            out_specs=(out, out),
            scratch_shapes=[pltpu.VMEM((2 * width, DK), BF)],
        ),
        out_shape=(shape, shape),
        compiler_params=params(12, "arbitrary"),
        cost_estimate=cost(4),
        name="finish",
    )(idx, o, qf, qb, o, qf, qb, line, gain, *deps)


def combine_kernel(routes_ref, logits_ref, *refs, chunks, experts):
    returned, out_ref = refs[:-1], refs[-1]
    rows = routes_ref.shape[0]
    expert_iota = lax.broadcasted_iota(jnp.int32, (rows, experts), 1)
    e0 = routes_ref[:, 0:1]
    e1 = routes_ref[:, 1:2]
    oh0 = (expert_iota == e0).astype(F32)
    oh1 = (expert_iota == e1).astype(F32)
    earlier = (
        lax.broadcasted_iota(jnp.int32, (rows, rows), 1)
        < lax.broadcasted_iota(jnp.int32, (rows, rows), 0)
    ).astype(F32)
    before = dot(earlier.astype(BF), (oh0 + oh1).astype(BF))
    slot0 = jnp.sum(oh0 * before, axis=1, keepdims=True).astype(jnp.int32)
    slot1 = jnp.sum(oh1 * (before + oh0), axis=1, keepdims=True).astype(jnp.int32)
    logits = logits_ref[...]
    gap = logits[:, 0:1] - logits[:, 1:2]

    def picked(expert, slot):
        total = 0.0
        for result, (first, count) in zip(returned, chunks):
            inside = (slot >= first) & (slot < first + count)
            place = jnp.where(inside, expert * count + slot - first, -1)
            lane_iota = lax.broadcasted_iota(jnp.int32, (rows, experts * count), 1)
            chosen = (lane_iota == place).astype(F32).astype(BF)
            total = total + dot(chosen, result[...])
        return total

    out_ref[...] = (
        picked(e0, slot0) * jax.nn.sigmoid(gap) + picked(e1, slot1) * jax.nn.sigmoid(-gap)
    ).astype(BF)


def combine(routes, logits, returned, experts):
    rows = routes.shape[0]
    cols = returned[0].shape[1]
    return pl.pallas_call(
        functools.partial(combine_kernel, chunks=((0, sum(n for _, n in CHUNKS)),), experts=experts),
        out_shape=jax.ShapeDtypeStruct((rows, cols), BF),
        in_specs=[pl.BlockSpec(memory_space=pltpu.VMEM) for _ in range(2 + len(returned))],
        out_specs=pl.BlockSpec(memory_space=pltpu.VMEM),
        compiler_params=params(12),
        cost_estimate=cost(4),
        name="combine",
    )(routes, logits, *returned)


def ring(count, shift):
    return [(i, (i + shift) % count) for i in range(count)]


def body(
    mix_tokens,
    mix_gain,
    w_query,
    w_forget_fwd,
    w_forget_bwd,
    w_value,
    decay_floor,
    decay_shift,
    head_gain,
    w_out,
    moe_tokens,
    moe_gain,
    routes,
    route_logits,
    w_expert_gate,
    w_expert_up,
    w_expert_down,
):
    experts = lax.axis_size(EP)
    groups = lax.axis_size("y")
    core, chip = lax.axis_index("c"), lax.axis_index("y")
    idx = jnp.stack([core, chip, lax.axis_index(EP)]).astype(jnp.int32)
    swap = [(0, 1), (1, 0)]
    wg, wu, wd = w_expert_gate[0], w_expert_up[0], w_expert_down[0]

    outgoing = dispatch(idx, moe_tokens, moe_gain[None], routes.T, experts)
    o, qf, qb, message, wg, wu, wd_theirs, wd_mine = local_sweeps(
        idx,
        mix_tokens,
        mix_gain[None],
        w_query,
        w_forget_fwd,
        w_forget_bwd,
        w_value,
        decay_floor[None],
        decay_shift,
        wg,
        wu,
        wd,
        experts,
        groups,
        deps=outgoing,
    )
    late_idx, qf = lax.optimization_barrier((idx, qf))
    late_idx = jnp.maximum(late_idx, 0)
    landed = []
    arrived = []
    for rows, (_, count) in zip(outgoing, CHUNKS):
        shaped = rows.reshape(experts, count, rows.shape[1])
        got = lax.all_to_all(shaped, EP, split_axis=0, concat_axis=0, tiled=True)
        arrived.append(got.reshape(rows.shape))
    arrived[-1], message = lax.optimization_barrier((arrived[-1], message))
    line = lax.all_to_all(message, EP, split_axis=0, concat_axis=0, tiled=True)
    for own in arrived:
        other = lax.ppermute(own, "c", swap)
        x = lax.optimization_barrier(jnp.concatenate([own, other], axis=1))
        hidden = (jax.nn.silu(dot(x, wg)) * dot(x, wu)).astype(BF)
        for_partner = dot(hidden, wd_theirs).astype(BF)
        received = lax.ppermute(for_partner, "c", swap)
        mine = lax.optimization_barrier(dot(hidden, wd_mine).astype(BF))
        cols = received.shape[1] // groups
        pair = [
            (
                mine[:, at : at + cols].astype(F32) + received[:, at : at + cols].astype(F32)
            ).astype(BF)
            for at in range(0, received.shape[1], cols)
        ]
        landed.append([pair[0]] + [lax.ppermute(pair[d], "y", ring(groups, d)) for d in (2, 1, 3)])
    keep, give = finish(late_idx, o, qf, qb, line, head_gain[None], groups, deps=tuple(pair[1:]))
    given = lax.ppermute(give, "c", swap)
    lower = jnp.where(core == 0, keep, given)
    upper = jnp.where(core == 0, given, keep)
    parts = [jnp.stack([lower[d], upper[d]]) for d in range(groups)]
    moved = [parts[0]] + [lax.ppermute(parts[d], "y", ring(groups, d)) for d in range(1, groups)]
    shaped = jnp.concatenate(
        [
            sum(part.astype(F32) for part in chunk).astype(BF).reshape(experts, -1, cols)
            for chunk in landed
        ],
        axis=1,
    )
    back = lax.all_to_all(shaped, EP, split_axis=0, concat_axis=0, tiled=True)
    returned = [back.reshape(-1, cols)]
    turned = [moved[0]] + moved[:0:-1]
    features = jnp.concatenate([part[i] for part in turned for i in range(2)], axis=1)
    start = lax.rem(groups - chip, groups) * (features.shape[1] // groups)
    features = lax.dynamic_slice_in_dim(
        jnp.concatenate([features, features], axis=1), start, features.shape[1], axis=1
    )
    mixed_out = dot(features, w_out).astype(BF)
    moe_out = combine(routes, route_logits, returned, experts)
    return (mixed_out, moe_out)


def solution(mesh):
    finer = Mesh(mesh.devices.reshape(4, 4, 4, 2), ALL)

    return jax.shard_map(
        body,
        mesh=finer,
        in_specs=(
            P(EP, None),
            P(),
            P(None, TP),
            P(None, TP),
            P(None, TP),
            P(None, TP),
            P(TP),
            P(EP, TP),
            P(),
            P(),
            P(EP, None),
            P(),
            P(EP, None),
            P(EP, None),
            P(EP, None, TP),
            P(EP, None, TP),
            P(EP, TP, None),
        ),
        out_specs=(P(ALL, None), P(EP, TP)),
        check_vma=False,
    )
```
